32 devices in a mesh: grp: 2 (over x), tp: 16 (over z, y, core).
Axes of the slice: x: 2, y: 2, z: 4, core: 2. Of those that a mesh axis runs over, the one named last changes fastest.
Arguments:
- tokens: bfloat16 [128, 2048], P('grp'), parts along dimension 0, may hold values from -6 to 6
- norm_gain: float32 [2, 2048], replicated, may hold values from 0.1 to 1.9
- query_weight: bfloat16 [2, 2048, 2048], P(None, 'tp'), may hold values from -0.125 to 0.125
- key_weight: bfloat16 [2, 2048, 2048], P(None, 'tp'), may hold values from -0.125 to 0.125
- value_weight: bfloat16 [2, 2048, 2048], P(None, 'tp'), may hold values from -0.125 to 0.125
- outgate_weight: bfloat16 [2, 2048, 2048], P(None, 'tp'), may hold values from -0.125 to 0.125
- gate_weight: bfloat16 [2, 2048, 16], replicated, may hold values from -0.125 to 0.125
- forget_bias: float32 [2, 8], replicated, may hold values from 0 to 4
- proj_weight: bfloat16 [2, 2048, 2048], P(None, 'tp'), may hold values from -0.125 to 0.125
- cell_state: float32 [2, 128, 2048, 256], P(None, 'grp', 'tp'), parts along dimension 1, may hold values from -0.3 to 0.3
- normalizer: float32 [2, 128, 2048], P(None, 'grp', 'tp'), parts along dimension 1, may hold values from -0.3 to 0.3
- stabilizer: float32 [2, 128, 8], P(None, 'grp'), parts along dimension 1, may hold values from -2 to 2
Outputs:
- mixed: bfloat16 [128, 2048], P('grp', 'tp'), parts along dimension 0
- new_cell: float32 [2, 128, 2048, 256], P(None, 'grp', 'tp'), parts along dimension 1
- new_normalizer: float32 [2, 128, 2048], P(None, 'grp', 'tp'), parts along dimension 1
- new_stabilizer: float32 [2, 128, 8], P(None, 'grp'), parts along dimension 1
The draws below stay inside these ranges and needn't reach their ends.
There are 2 independent parts, one for each index of `grp`. The reference program is written for one: setup_inputs(seed, part) draws one part's arguments, and reference() takes and returns one part's arrays. A program takes and returns all parts, laid end to end along the dimension named above; an argument that names none is the same for every part. Nothing has to cross between parts.
All inputs are finite; a program needn't handle non-finite values.
Results may differ from the reference program's by a relative error of at most 0.025.
Values may be sent and summed in bfloat16 or wider, within the bound.
A program may use at most 64 MiB of HBM per device.

```python
import jax
import jax.numpy as jnp
from jax import lax

D = 2048
DH = 256
HEADS = 8
LAYERS = 2
BATCH = 64


def block_levels(rng, dims, split, low, largest):
    loudness = 1.0
    for axis_at, parts in split:
        heights = jax.random.uniform(jax.random.fold_in(jax.random.fold_in(rng, 6), axis_at), (parts,), jnp.float32, low / len(split), largest / len(split))
        loudness = loudness * jnp.repeat(jnp.exp(heights), dims[axis_at] // parts).reshape((-1,) + (1,) * (len(dims) - 1 - axis_at))
    return loudness


def centred(key, shape, width, most, shards=(), kind=jnp.bfloat16):
    entries = jax.random.normal(key, shape, jnp.float32) * width
    if len(shards) > 0:
        entries = block_levels(key, shape, shards, -0.22, 0.18) * entries
    return jnp.clip(entries, min=-most, max=most).astype(kind)


def setup_inputs(seed: int = 0, part: int = 0) -> dict:
    key_list = jax.random.split(jax.random.key(seed), 13)
    own_keys = jax.random.split(jax.random.fold_in(key_list[12], part), 13)
    tokens = centred(own_keys[0], (BATCH, D), 1.0, 6.0)
    norm_gain = jnp.clip(1.0 + 0.18 * jax.random.normal(key_list[1], (LAYERS, D), jnp.float32), 0.1, 1.9)
    query_weight = centred(key_list[2], (LAYERS, D, D), D ** -0.5, 0.125, ((1, 16),))
    key_weight = centred(key_list[3], (LAYERS, D, D), D ** -0.5, 0.125, ((1, 16),))
    value_weight = centred(key_list[4], (LAYERS, D, D), D ** -0.5, 0.125, ((1, 16),))
    outgate_weight = centred(key_list[5], (LAYERS, D, D), D ** -0.5, 0.125, ((1, 16),))
    gate_weight = centred(key_list[6], (LAYERS, D, 2 * HEADS), D ** -0.5, 0.125)
    forget_bias = jnp.clip(jax.random.uniform(key_list[7], (LAYERS, HEADS), jnp.float32, 0.0, 4.0), 0.0, 4.0)
    proj_weight = centred(key_list[8], (LAYERS, D, D), D ** -0.5, 0.125, ((1, 16),))
    cell_state = centred(own_keys[9], (LAYERS, BATCH, D, DH), 0.05, 0.3, ((2, 16),), jnp.float32)
    normalizer = centred(own_keys[10], (LAYERS, BATCH, D), 0.05, 0.3, ((2, 16),), jnp.float32)
    stabilizer = jnp.clip(jax.random.uniform(own_keys[11], (LAYERS, BATCH, HEADS), jnp.float32, -2.0, 2.0), -2.0, 2.0)
    return {"tokens": tokens, "norm_gain": norm_gain, "query_weight": query_weight, "key_weight": key_weight, "value_weight": value_weight, "outgate_weight": outgate_weight, "gate_weight": gate_weight, "forget_bias": forget_bias, "proj_weight": proj_weight, "cell_state": cell_state, "normalizer": normalizer, "stabilizer": stabilizer}


epsilon = 1e-06

def project(normed, weight):
    return lax.dot_general(normed, weight, (((1,), (1,)), ((), ())), preferred_element_type=jnp.float32)

def one_cell(current, gain, w_query, w_key, w_value, w_outgate, w_gates, bias_forget, w_proj, cell, norm_vec, stab):
    batch = current.shape[0]
    heads = D // DH
    cur_f = current.astype(jnp.float32)
    normed = (cur_f * lax.rsqrt(lax.optimization_barrier(jnp.mean(cur_f * cur_f, axis=-1, keepdims=True)) + epsilon) * gain).astype(jnp.bfloat16)
    query = project(normed, w_query).astype(jnp.bfloat16)
    keys = (project(normed, w_key) * DH ** (-0.5)).astype(jnp.bfloat16)
    values = project(normed, w_value).astype(jnp.bfloat16)
    outgate = project(normed, w_outgate).astype(jnp.bfloat16)
    gates = jnp.dot(normed, w_gates, preferred_element_type=jnp.float32)
    in_gate = gates[:, :heads]
    log_forget = jax.nn.log_sigmoid(gates[:, heads:] + bias_forget)
    new_stab = jnp.maximum(log_forget + stab, in_gate)
    decay = jnp.exp(log_forget + stab - new_stab)
    weight_in = jnp.exp(in_gate - new_stab)
    q_heads = query.astype(jnp.float32).reshape(batch, heads, DH)
    k_heads = keys.astype(jnp.float32).reshape(batch, heads, DH)
    v_heads = values.astype(jnp.float32).reshape(batch, heads, DH)
    old_cell = cell.reshape(batch, heads, DH, DH)
    outer = v_heads[:, :, :, None] * k_heads[:, :, None, :]
    new_cell = decay[:, :, None, None] * old_cell + weight_in[:, :, None, None] * outer
    new_norm = decay[:, :, None] * norm_vec.reshape(batch, heads, DH) + weight_in[:, :, None] * k_heads
    numer = jnp.einsum('bhk,bhek->bhe', q_heads, new_cell, precision=lax.Precision.HIGHEST)
    denom = lax.optimization_barrier(jnp.sum(q_heads * new_norm, axis=-1))
    readout = numer / jnp.maximum(jnp.abs(denom), jnp.exp(-new_stab))[:, :, None]
    branch = (jax.nn.sigmoid(outgate.astype(jnp.float32)) * readout.reshape(batch, D)).astype(jnp.bfloat16)
    result = (cur_f + project(branch, w_proj)).astype(jnp.bfloat16)
    return (result, new_cell.reshape(batch, D, DH), new_norm.reshape(batch, D), new_stab)

def reference(tokens, norm_gain, query_weight, key_weight, value_weight, outgate_weight, gate_weight, forget_bias, proj_weight, cell_state, normalizer, stabilizer):
    current = tokens
    cells = []
    norms = []
    stabs = []
    for layer in range(LAYERS):
        current, new_cell, new_norm, new_stab = one_cell(current, norm_gain[layer], query_weight[layer], key_weight[layer], value_weight[layer], outgate_weight[layer], gate_weight[layer], forget_bias[layer], proj_weight[layer], cell_state[layer], normalizer[layer], stabilizer[layer])
        cells.append(new_cell)
        norms.append(new_norm)
        stabs.append(new_stab)
    return (current, jnp.stack(cells), jnp.stack(norms), jnp.stack(stabs))
```

```python
import functools

import jax
import jax.numpy as jnp
from jax import lax
from jax.experimental import pallas as pl
from jax.experimental.pallas import tpu as pltpu
from jax.sharding import PartitionSpec as P

D = 2048
DH = 256
LAYERS = 2


epsilon = 1e-06


def from_partner(value, axis, apart):
    mask = 2**apart
    pairs = [(source, source ^ mask) for source in range(lax.axis_size(axis))]
    return lax.ppermute(value, axis, pairs)


def project(normed, weight):
    return lax.dot_general(
        normed, weight, (((1,), (1,)), ((), ())), preferred_element_type=jnp.float32
    )


def split_pieces(value):
    high = lax.optimization_barrier(value.astype(jnp.bfloat16))
    rest = value - high.astype(jnp.float32)
    middle = lax.optimization_barrier(rest.astype(jnp.bfloat16))
    lowest = (rest - middle.astype(jnp.float32)).astype(jnp.bfloat16)
    return jnp.stack([high, middle, lowest], axis=1)


def join_pieces(pieces):
    return jnp.sum(pieces.astype(jnp.float32), axis=-1)


def combine_halves(mine, theirs, lower):
    return jnp.where(
        lower, jnp.concatenate([mine, theirs], axis=1), jnp.concatenate([theirs, mine], axis=1)
    )


def one_cell(
    current,
    gain,
    w_query,
    w_key,
    w_value,
    w_outgate,
    w_gates,
    bias_forget,
    w_proj,
    cell,
    norm_vec,
    stab,
):
    heads = D // DH
    ncols = w_query.shape[0]
    group = DH // ncols
    device = lax.axis_index("tp")
    head = device // group
    cur_f = current.astype(jnp.float32)
    normed = (
        cur_f * lax.rsqrt(jnp.mean(cur_f * cur_f, axis=-1, keepdims=True) + epsilon) * gain
    ).astype(jnp.bfloat16)
    query = project(normed, w_query).astype(jnp.bfloat16)
    keys = (project(normed, w_key) * DH ** (-0.5)).astype(jnp.bfloat16)
    values = project(normed, w_value).astype(jnp.bfloat16)
    outgate = project(normed, w_outgate).astype(jnp.bfloat16)
    gates = jnp.dot(normed, w_gates, preferred_element_type=jnp.float32)
    in_gate = gates[:, :heads]
    log_forget = jax.nn.log_sigmoid(gates[:, heads:] + bias_forget)
    new_stab = jnp.maximum(log_forget + stab, in_gate)
    decay = jnp.exp(log_forget + stab - new_stab)
    weight_in = jnp.exp(in_gate - new_stab)
    select = (jnp.arange(heads) == head).astype(jnp.float32)
    my_decay = jnp.sum(decay * select, axis=-1)
    my_weight = jnp.sum(weight_in * select, axis=-1)
    my_stab = jnp.sum(new_stab * select, axis=-1)
    new_norm = my_decay[:, None] * norm_vec + my_weight[:, None] * keys.astype(jnp.float32)
    den_part = jnp.sum(query.astype(jnp.float32) * new_norm, axis=-1)
    q_head, k_head = (query, keys)
    denom = den_part
    for bit in range(group.bit_length() - 1):
        other_q, other_k, other_pieces = from_partner(
            (q_head, k_head, split_pieces(denom)), "tp", bit
        )
        lower = device // 2**bit % 2 == 0
        q_head = combine_halves(q_head, other_q, lower)
        k_head = combine_halves(k_head, other_k, lower)
        denom = denom + join_pieces(other_pieces)
    outer = values.astype(jnp.float32)[:, :, None] * k_head.astype(jnp.float32)[:, None, :]
    new_cell = my_decay[:, None, None] * cell + my_weight[:, None, None] * outer
    numer = jnp.einsum(
        "bk,bek->be", q_head.astype(jnp.float32), new_cell, precision=lax.Precision.HIGHEST
    )
    readout = numer / jnp.maximum(jnp.abs(denom), jnp.exp(-my_stab))[:, None]
    branch = (jax.nn.sigmoid(outgate.astype(jnp.float32)) * readout).astype(jnp.bfloat16)
    summed = project(lax.all_gather(branch, "tp", axis=1, tiled=True), w_proj)
    own_input = lax.dynamic_slice_in_dim(cur_f, device * ncols, ncols, 1)
    result = (own_input + summed).astype(jnp.bfloat16)
    return (result, new_cell, new_norm, new_stab)


def body(
    tokens,
    norm_gain,
    query_weight,
    key_weight,
    value_weight,
    outgate_weight,
    gate_weight,
    forget_bias,
    proj_weight,
    cell_state,
    normalizer,
    stabilizer,
):
    current = tokens
    cells = []
    norms = []
    stabs = []
    result = tokens
    for layer in range(LAYERS):
        result, new_cell, new_norm, new_stab = one_cell(
            current,
            norm_gain[layer],
            query_weight[layer],
            key_weight[layer],
            value_weight[layer],
            outgate_weight[layer],
            gate_weight[layer],
            forget_bias[layer],
            proj_weight[layer],
            cell_state[layer],
            normalizer[layer],
            stabilizer[layer],
        )
        cells.append(new_cell)
        norms.append(new_norm)
        stabs.append(new_stab)
        if layer + 1 < LAYERS:
            current = lax.all_gather(result, "tp", axis=1, tiled=True)
    return (result, jnp.stack(cells), jnp.stack(norms), jnp.stack(stabs))


NT = (((1,), (1,)), ((), ()))
CELL_CHUNKS = 4
MAIN_VMEM = 24 * 2**20
LAST_VMEM = 6 * 2**20


def flip(index, mask):
    result = index
    bit = 1
    while bit <= mask:
        if mask & bit:
            result = result + bit - 2 * bit * lax.rem(lax.div(index, bit), 2)
        bit *= 2
    return result


def fetch(source, target, sem):
    copy = pltpu.make_async_copy(source, target, sem)
    copy.start()
    return copy


def push(source, dest, target, send, recv):
    copy = pltpu.make_async_remote_copy(
        src_ref=source,
        dst_ref=dest,
        send_sem=send,
        recv_sem=recv,
        device_id={"tp": target},
        device_id_type=pl.DeviceIdType.MESH,
    )
    copy.start()
    return copy


def arrived(buffer, recv):
    pltpu.make_async_copy(buffer, buffer, recv).wait()


def greet_all(n, me):
    barrier = pltpu.get_barrier_semaphore()
    for i in range(1, n):
        pl.semaphore_signal(
            barrier,
            inc=1,
            device_id={"tp": lax.rem(me + i, n)},
            device_id_type=pl.DeviceIdType.MESH,
        )
    return barrier


def read_rows(cell_rows, queries, numer, start, rows):
    ncols = numer.shape[1]
    row = lax.broadcasted_iota(jnp.int32, (rows, ncols), 0)
    total = jnp.zeros((rows, ncols), jnp.float32)
    for b in range(rows):
        block = cell_rows(start + b).astype(jnp.bfloat16)
        product = lax.dot_general(queries, block, NT, preferred_element_type=jnp.float32)
        total = jnp.where(row == b, product, total)
    numer[pl.ds(start, rows), :] = total


def send_half(half, chip, core, chips, rows, source, dest, send, recv):
    me = chip * 2 + core
    return [
        push(
            source.at[pl.ds(half * rows, rows)],
            dest.at[me],
            flip(chip, m) * 2 + half,
            send.at[half, m],
            recv.at[m, core],
        )
        for m in range(chips - 1, 0, -1)
    ]


def gather_project(chip, core, chips, rows, source, dest, send, recv, weights, copies):
    me = chip * 2 + core
    partner = chip * 2 + 1 - core
    ncols = dest.shape[2]
    copies.append(
        push(
            source.at[pl.ds(pl.multiple_of((1 - core) * rows, rows), rows)],
            dest.at[me],
            partner,
            send.at[0, 0],
            recv.at[0, core],
        )
    )
    dest[me] = source[pl.ds(pl.multiple_of(core * rows, rows), rows), :]
    total = jnp.zeros((rows, 2 * ncols), jnp.float32)
    for m in range(chips):
        other = flip(chip, m)
        if m == 0:
            arrived(dest.at[partner], recv.at[0, 1 - core])
        else:
            for c in range(2):
                arrived(dest.at[other * 2 + c], recv.at[m, c])
        block = jnp.concatenate([dest[other * 2], dest[other * 2 + 1]], axis=1)
        part = weights[:, pl.ds(pl.multiple_of(other * 2 * ncols, 2 * ncols), 2 * ncols)]
        total = total + lax.dot_general(block, part, NT, preferred_element_type=jnp.float32)
    return total


def cells_kernel(
    n,
    tokens,
    norm_gain,
    w_query,
    w_key,
    w_value,
    w_outgate,
    w_gates,
    bias_forget,
    w_proj,
    cell,
    norm_vec,
    stab,
    cell_buf,
    new_norm,
    new_stab,
    wv_buf,
    key_buf,
    decay_buf,
    q_out,
    inner_out,
    den_out,
    gate_out,
    own_out,
    tok_buf,
    gain_buf,
    weights,
    wide,
    proj_buf,
    gate_buf,
    bias_buf,
    stab_buf,
    norm_buf,
    pair_buf,
    send_buf,
    branch_buf,
    result_buf,
    whole_buf,
    swap_buf,
    swap_out,
    gates_buf,
    numer_buf,
    small_sem,
    weight_sem,
    wide_sem,
    cell_sem,
    pair_send,
    pair_recv,
    branch_send,
    branch_recv,
    result_send,
    result_recv,
):
    layers, batch, ncols, dh = cell.shape
    width = tokens.shape[1]
    heads = stab.shape[1]
    rows = batch // CELL_CHUNKS
    half = batch // 2
    chips = n // 2
    me = lax.axis_index("tp")
    core = lax.rem(me, 2)
    chip = lax.div(me, 2)
    partner = chip * 2 + 1 - core
    barrier = greet_all(n, me)

    tok_copy = fetch(tokens, tok_buf, small_sem.at[0])
    gain_copy = fetch(norm_gain, gain_buf, small_sem.at[1])
    names = [w_query, w_key, w_value, w_outgate]
    weight_copies = [
        fetch(names[i].at[0], weights.at[pl.ds(i * ncols, ncols)], weight_sem.at[i])
        for i in range(4)
    ]
    small = [
        fetch(w_gates, gate_buf, small_sem.at[2]),
        fetch(bias_forget, bias_buf, small_sem.at[3]),
        fetch(stab, stab_buf, small_sem.at[4]),
    ]
    norm_copy = fetch(norm_vec, norm_buf.at[core], small_sem.at[5])

    def fetch_cell(layer):
        return [
            fetch(
                cell.at[layer, pl.ds(c * rows, rows)],
                cell_buf.at[layer, pl.ds(c * rows, rows)],
                cell_sem.at[layer, c],
            )
            for c in range(CELL_CHUNKS)
        ]

    def own_rows(ref, i):
        return ref.at[pl.ds(pl.multiple_of(i * 2 * ncols + core * ncols, ncols), ncols)]

    def scale(gates, layer):
        in_gate = gates[:, :heads]
        forget = gates[:, heads : 2 * heads] + bias_buf[pl.ds(layer, 1), :]
        log_forget = jnp.minimum(forget, 0.0) - jnp.log1p(jnp.exp(-jnp.abs(forget)))
        old_stab = stab_buf[layer].T
        next_stab = jnp.maximum(log_forget + old_stab, in_gate)
        new_stab[layer] = next_stab.T
        mine = lax.broadcasted_iota(jnp.int32, (batch, heads), 1) == chip

        def pick(entry):
            return jnp.sum(jnp.where(mine, entry, 0.0), axis=-1, keepdims=True)

        my_stab = pick(next_stab)
        my_decay = jnp.exp(pick(log_forget + old_stab) - my_stab)
        my_weight = jnp.exp(pick(in_gate) - my_stab)
        return my_stab, my_decay, my_weight

    def finish_head(layer, q_head, k_head, my_stab, my_decay, my_weight):
        n_head = jnp.concatenate([norm_buf[j, layer] for j in range(2)], axis=1)
        denom = jnp.sum(
            q_head * (my_decay * n_head + my_weight * k_head), axis=-1, keepdims=True
        )
        inner = jnp.sum(q_head * k_head, axis=-1, keepdims=True)
        return inner, jnp.maximum(jnp.abs(denom), jnp.exp(-my_stab))

    tok_copy.wait()
    gain_copy.wait()
    current = tok_buf[...].astype(jnp.float32)
    mean = jnp.sum(current * current, axis=-1, keepdims=True) * (1.0 / width)
    normed = (current * lax.rsqrt(mean + epsilon) * gain_buf[0:1, :]).astype(jnp.bfloat16)
    weight_copies[0].wait()
    weight_copies[1].wait()
    both = lax.dot_general(
        normed, weights[: 2 * ncols], NT, preferred_element_type=jnp.float32
    )
    pair_buf[core, 0] = both[:, :ncols].astype(jnp.bfloat16)
    key = (both[:, ncols:] * dh ** (-0.5)).astype(jnp.bfloat16)
    pair_buf[core, 1] = key
    weight_copies[2].wait()
    weight_copies[3].wait()
    for copy in small:
        copy.wait()
    norm_copy.wait()
    proj_copy = fetch(w_proj.at[0], own_rows(proj_buf, 0), small_sem.at[6])
    cell_copies = fetch_cell(0)
    pl.semaphore_wait(barrier, n - 1)
    pair_copies = [
        push(pair_buf.at[core], pair_buf.at[core], partner, pair_send.at[0], pair_recv.at[0]),
        push(norm_buf.at[core], norm_buf.at[core], partner, pair_send.at[1], pair_recv.at[1]),
    ]
    both = lax.dot_general(
        normed, weights[2 * ncols :], NT, preferred_element_type=jnp.float32
    )
    value = both[:, :ncols].astype(jnp.bfloat16).astype(jnp.float32)
    gate = jax.nn.sigmoid(both[:, ncols:].astype(jnp.bfloat16).astype(jnp.float32))
    gates = lax.dot_general(normed, gate_buf[0], NT, preferred_element_type=jnp.float32)
    my_stab, my_decay, my_weight = scale(gates, 0)
    new_norm[0] = my_decay * norm_buf[core, 0] + my_weight * key.astype(jnp.float32)
    weighted = my_weight * value
    wv_buf[0] = weighted
    decay_buf[0] = jnp.broadcast_to(my_decay, (batch, ncols))
    arrived(pair_buf.at[1 - core], pair_recv.at[0])
    arrived(norm_buf.at[1 - core], pair_recv.at[1])
    proj_copy.wait()
    pair_copies.append(
        push(own_rows(proj_buf, 0), own_rows(proj_buf, 0), partner, pair_send.at[2], pair_recv.at[2])
    )
    q_head = jnp.concatenate([pair_buf[j, 0] for j in range(2)], axis=1).astype(jnp.float32)
    k_head = jnp.concatenate([pair_buf[j, 1] for j in range(2)], axis=1).astype(jnp.float32)
    key_buf[0] = k_head
    inner, den = finish_head(0, q_head, k_head, my_stab, my_decay, my_weight)

    branch_copies = []
    for h in range(2):
        for c in range(h * CELL_CHUNKS // 2, (h + 1) * CELL_CHUNKS // 2):
            cell_copies[c].wait()
            queries = jnp.concatenate(
                [pair_buf[j, 0, pl.ds(c * rows, rows), :] for j in range(2)], axis=1
            )
            read_rows(lambda b: cell_buf[0, b], queries, numer_buf, c * rows, rows)
        part = slice(h * half, (h + 1) * half)
        numer = my_decay[part] * numer_buf[part, :] + weighted[part] * inner[part]
        send_buf[part, :] = (gate[part] * (numer / den[part])).astype(jnp.bfloat16)
        branch_copies += send_half(
            h, chip, core, chips, half, send_buf, branch_buf, branch_send, branch_recv
        )
    wide_copies = [
        fetch(names[i].at[1], own_rows(wide, i), wide_sem.at[i]) for i in range(4)
    ]
    cell_copies = fetch_cell(1)
    arrived(
        proj_buf.at[pl.ds(pl.multiple_of((1 - core) * ncols, ncols), ncols)], pair_recv.at[2]
    )
    wide_pushes = []
    for i in range(4):
        wide_copies[i].wait()
        wide_pushes.append(
            push(
                own_rows(wide, i),
                own_rows(wide, i),
                partner,
                pair_send.at[3 + i],
                pair_recv.at[3 + i],
            )
        )
    summed = gather_project(
        chip,
        core,
        chips,
        half,
        send_buf,
        branch_buf,
        branch_send,
        branch_recv,
        proj_buf,
        branch_copies,
    )
    my_rows = pl.ds(pl.multiple_of(core * half, half), half)
    my_cols = pl.ds(pl.multiple_of(chip * 2 * ncols, 2 * ncols), 2 * ncols)
    result = (tok_buf[my_rows, my_cols].astype(jnp.float32) + summed).astype(jnp.bfloat16)
    own_out[...] = result
    result_buf[chip] = result
    result_copies = [
        push(
            result_buf.at[chip],
            result_buf.at[chip],
            flip(chip, m) * 2 + core,
            result_send.at[m],
            result_recv.at[m],
        )
        for m in range(chips - 1, 0, -1)
    ]

    for i in range(4):
        arrived(
            wide.at[pl.ds(pl.multiple_of(i * 2 * ncols + (1 - core) * ncols, ncols), ncols)],
            pair_recv.at[3 + i],
        )
    total = jnp.zeros((half, 8 * ncols), jnp.float32)
    gates = jnp.zeros((half, 2 * heads), jnp.float32)
    square = jnp.zeros((half, 1), jnp.float32)
    for m in range(chips):
        other = flip(chip, m)
        if m:
            arrived(result_buf.at[other], result_recv.at[m])
        cols = pl.ds(pl.multiple_of(other * 2 * ncols, 2 * ncols), 2 * ncols)
        block = result_buf[other].astype(jnp.float32)
        square = square + jnp.sum(block * block, axis=-1, keepdims=True)
        block = (block * gain_buf[1:2, cols]).astype(jnp.bfloat16)
        total = total + lax.dot_general(
            block, wide[:, cols], NT, preferred_element_type=jnp.float32
        )
        gates = gates + lax.dot_general(
            block, gate_buf[1, :, cols], NT, preferred_element_type=jnp.float32
        )
    root = lax.rsqrt(square * (1.0 / width) + epsilon)
    total = total * root
    query = total[:, : 2 * ncols].astype(jnp.bfloat16)
    key = (total[:, 2 * ncols : 4 * ncols] * dh ** (-0.5)).astype(jnp.bfloat16)
    whole_buf[...] = total[:, 4 * ncols :].astype(jnp.bfloat16)
    for target, side in ((swap_buf.at[core], core), (swap_out, 1 - core)):
        target[:, : 2 * ncols] = query
        target[:, 2 * ncols : 4 * ncols] = key
        for i in range(2):
            target[:, (4 + i) * ncols : (5 + i) * ncols] = whole_buf[
                :, pl.ds(pl.multiple_of(i * 2 * ncols + side * ncols, ncols), ncols)
            ]
    gates_buf[core] = jnp.concatenate(
        [gates * root, jnp.zeros((half, ncols - 2 * heads), jnp.float32)], axis=1
    )
    pair_copies += [
        push(swap_out, swap_buf.at[core], partner, pair_send.at[7], pair_recv.at[7]),
        push(gates_buf.at[core], gates_buf.at[core], partner, pair_send.at[8], pair_recv.at[8]),
    ]
    for copy in branch_copies + wide_pushes + result_copies:
        copy.wait_send()
    for copy in cell_copies:
        copy.wait()
    arrived(swap_buf.at[1 - core], pair_recv.at[7])
    arrived(gates_buf.at[1 - core], pair_recv.at[8])

    def both_halves(part):
        return jnp.concatenate([swap_buf[j, :, part] for j in range(2)], axis=0)

    gates = jnp.concatenate([gates_buf[j] for j in range(2)], axis=0)
    my_stab, my_decay, my_weight = scale(gates, 1)
    queries = both_halves(slice(0, 2 * ncols))
    q_out[...] = queries
    q_head = queries.astype(jnp.float32)
    k_head = both_halves(slice(2 * ncols, 4 * ncols)).astype(jnp.float32)
    key_buf[1] = k_head
    key = both_halves(pl.ds(pl.multiple_of((2 + core) * ncols, ncols), ncols))
    new_norm[1] = my_decay * norm_buf[core, 1] + my_weight * key.astype(jnp.float32)
    weighted = my_weight * both_halves(slice(4 * ncols, 5 * ncols)).astype(jnp.float32)
    wv_buf[1] = weighted
    decay_buf[1] = jnp.broadcast_to(my_decay, (batch, ncols))
    gate_out[...] = jax.nn.sigmoid(both_halves(slice(5 * ncols, 6 * ncols)).astype(jnp.float32))
    inner, den = finish_head(1, q_head, k_head, my_stab, my_decay, my_weight)
    inner_out[...] = weighted * inner
    den_out[...] = jnp.broadcast_to(den, (batch, ncols))
    for copy in pair_copies:
        copy.wait_send()


def last_kernel(
    n,
    cell_buf,
    queries,
    decay,
    inner,
    den,
    gate,
    own,
    _,
    w_proj,
    mixed,
    proj_buf,
    send_buf,
    branch_buf,
    swap_buf,
    swap_out,
    numer_buf,
    proj_sem,
    pair_send,
    pair_recv,
    branch_send,
    branch_recv,
):
    layers, batch, ncols, dh = cell_buf.shape
    last = layers - 1
    rows = batch // CELL_CHUNKS
    half = batch // 2
    chips = n // 2
    me = lax.axis_index("tp")
    core = lax.rem(me, 2)
    chip = lax.div(me, 2)
    partner = chip * 2 + 1 - core
    barrier = greet_all(n, me)
    own_part = proj_buf.at[pl.ds(pl.multiple_of(core * ncols, ncols), ncols)]
    proj_copy = fetch(w_proj.at[last], own_part, proj_sem)
    copies = []
    for h in range(2):
        for c in range(h * CELL_CHUNKS // 2, (h + 1) * CELL_CHUNKS // 2):
            read_rows(
                lambda b: cell_buf[last, b],
                queries[pl.ds(c * rows, rows), :],
                numer_buf,
                c * rows,
                rows,
            )
        part = slice(h * half, (h + 1) * half)
        numer = decay[last, part, :] * numer_buf[part, :] + inner[part, :]
        send_buf[part, :] = (gate[part, :] * (numer / den[part, :])).astype(jnp.bfloat16)
        if h == 0:
            pl.semaphore_wait(barrier, n - 1)
        copies += send_half(
            h, chip, core, chips, half, send_buf, branch_buf, branch_send, branch_recv
        )
    proj_copy.wait()
    pair_copies = [push(own_part, own_part, partner, pair_send.at[0], pair_recv.at[0])]
    arrived(
        proj_buf.at[pl.ds(pl.multiple_of((1 - core) * ncols, ncols), ncols)], pair_recv.at[0]
    )
    summed = gather_project(
        chip,
        core,
        chips,
        half,
        send_buf,
        branch_buf,
        branch_send,
        branch_recv,
        proj_buf,
        copies,
    )
    result = (own[...].astype(jnp.float32) + summed).astype(jnp.bfloat16)
    swap_buf[...] = result
    swap_out[core] = swap_buf[:, pl.ds(pl.multiple_of((1 - core) * ncols, ncols), ncols)]
    pair_copies.append(
        push(swap_out.at[core], swap_out.at[2 + core], partner, pair_send.at[1], pair_recv.at[1])
    )
    mixed[pl.ds(pl.multiple_of(core * half, half), half), :] = swap_buf[
        :, pl.ds(pl.multiple_of(core * ncols, ncols), ncols)
    ]
    for copy in copies:
        copy.wait_send()
    arrived(swap_out.at[3 - core], pair_recv.at[1])
    mixed[pl.ds(pl.multiple_of((1 - core) * half, half), half), :] = swap_out[3 - core]
    for copy in pair_copies:
        copy.wait_send()


def fused_body(n, *args):
    (tokens, norm_gain, w_query, _, _, _, w_gates, bias_forget, _, cell, norm_vec, stab) = args
    layers, batch, ncols, dh = cell.shape
    width = tokens.shape[1]
    half = batch // 2
    chips = n // 2
    w_gates = jnp.swapaxes(w_gates, 1, 2)
    stab = jnp.swapaxes(stab, 1, 2)
    args = args[:6] + (w_gates,) + args[7:11] + (stab,)
    args = [pltpu.with_memory_space_constraint(arg, pltpu.HBM) for arg in args]
    bf16, f32 = jnp.bfloat16, jnp.float32
    vmem = pl.BlockSpec(memory_space=pltpu.VMEM)
    hbm = pl.BlockSpec(memory_space=pltpu.HBM)
    dma = pltpu.SemaphoreType.DMA
    rows = jax.ShapeDtypeStruct((batch, ncols), f32)
    held, new_norm, new_stab, weighted, keys, decay, queries, inner, den, gate, own = pl.pallas_call(
        functools.partial(cells_kernel, n),
        out_shape=(
            pltpu.VMEM(cell.shape, f32),
            jax.ShapeDtypeStruct(norm_vec.shape, f32),
            jax.ShapeDtypeStruct(stab.shape, f32),
            jax.ShapeDtypeStruct((layers, batch, ncols), f32),
            jax.ShapeDtypeStruct((layers, batch, dh), f32),
            jax.ShapeDtypeStruct((layers, batch, ncols), f32),
            jax.ShapeDtypeStruct((batch, dh), bf16),
            rows,
            rows,
            rows,
            jax.ShapeDtypeStruct((half, dh), bf16),
        ),
        in_specs=[hbm] * len(args),
        out_specs=(vmem,) * 11,
        scratch_shapes=[
            pltpu.VMEM(tokens.shape, bf16),
            pltpu.VMEM(norm_gain.shape, f32),
            pltpu.VMEM((4 * ncols, width), bf16),
            pltpu.VMEM((8 * ncols, width), bf16),
            pltpu.VMEM((2 * ncols, width), bf16),
            pltpu.VMEM(w_gates.shape, bf16),
            pltpu.VMEM(bias_forget.shape, f32),
            pltpu.VMEM(stab.shape, f32),
            pltpu.VMEM((2,) + norm_vec.shape, f32),
            pltpu.VMEM((2, 2, batch, ncols), bf16),
            pltpu.VMEM((batch, ncols), bf16),
            pltpu.VMEM((n, half, ncols), bf16),
            pltpu.VMEM((chips, half, 2 * ncols), bf16),
            pltpu.VMEM((half, 4 * ncols), bf16),
            pltpu.VMEM((2, half, 6 * ncols), bf16),
            pltpu.VMEM((half, 6 * ncols), bf16),
            pltpu.VMEM((2, half, ncols), f32),
            pltpu.VMEM((batch, ncols), f32),
            dma((7,)),
            dma((4,)),
            dma((4,)),
            dma((layers, CELL_CHUNKS)),
            dma((9,)),
            dma((9,)),
            dma((2, chips)),
            dma((chips, 2)),
            dma((chips,)),
            dma((chips,)),
        ],
        compiler_params=pltpu.CompilerParams(
            collective_id=0, has_side_effects=True, vmem_limit_bytes=MAIN_VMEM
        ),
        name="cells",
    )(*args)
    new_cell = (
        decay[:, :, :1, None] * held + weighted[:, :, :, None] * keys[:, :, None, :]
    )
    mixed = pl.pallas_call(
        functools.partial(last_kernel, n),
        out_shape=jax.ShapeDtypeStruct((batch, ncols), bf16),
        in_specs=[vmem] * 8 + [hbm],
        out_specs=vmem,
        scratch_shapes=[
            pltpu.VMEM((2 * ncols, width), bf16),
            pltpu.VMEM((batch, ncols), bf16),
            pltpu.VMEM((n, half, ncols), bf16),
            pltpu.VMEM((half, 2 * ncols), bf16),
            pltpu.VMEM((4, half, ncols), bf16),
            pltpu.VMEM((batch, ncols), f32),
            dma,
            dma((2,)),
            dma((2,)),
            dma((2, chips)),
            dma((chips, 2)),
        ],
        compiler_params=pltpu.CompilerParams(
            collective_id=1, has_side_effects=True, vmem_limit_bytes=LAST_VMEM
        ),
        cost_estimate=pl.CostEstimate(
            flops=5 * 10**10, bytes_accessed=10**6, transcendentals=0
        ),
        name="last",
    )(held, queries, decay, inner, den, gate, own, new_cell[0, 0, :8, :128], args[8])
    mixed, new_norm, new_stab = write_small(mixed, new_norm, new_stab)
    return mixed, new_cell, new_norm, jnp.swapaxes(new_stab, 1, 2)


def write_kernel(*refs):
    half = len(refs) // 2
    sems = refs[-1]
    copies = [
        pltpu.make_async_copy(refs[i], refs[half + i], sems.at[i]) for i in range(half)
    ]
    for copy in copies:
        copy.start()
    for copy in copies:
        copy.wait()


def write_small(*arrays):
    return pl.pallas_call(
        write_kernel,
        out_shape=[jax.ShapeDtypeStruct(x.shape, x.dtype) for x in arrays],
        in_specs=[pl.BlockSpec(memory_space=pltpu.VMEM)] * len(arrays),
        out_specs=[pl.BlockSpec(memory_space=pltpu.HBM)] * len(arrays),
        scratch_shapes=[pltpu.SemaphoreType.DMA((len(arrays),))],
        compiler_params=pltpu.CompilerParams(vmem_limit_bytes=2**20),
        name="write",
    )(*arrays)


def whole_body(*args):
    n = lax.axis_size("tp")
    layers, batch, ncols, dh = args[9].shape
    heads = args[11].shape[2]
    if (
        layers == 2
        and n == 2 * heads
        and n & (n - 1) == 0
        and ncols % 128 == 0
        and dh == 2 * ncols
        and batch % (16 * CELL_CHUNKS) == 0
    ):
        return fused_body(n, *args)
    return body(*args)


def solution(mesh):
    return jax.shard_map(
        whole_body,
        mesh=mesh,
        in_specs=(
            P("grp", None),
            P(),
            P(None, "tp", None),
            P(None, "tp", None),
            P(None, "tp", None),
            P(None, "tp", None),
            P(),
            P(),
            P(None, "tp", None),
            P(None, "grp", "tp", None),
            P(None, "grp", "tp"),
            P(None, "grp", None),
        ),
        out_specs=(
            P("grp", "tp"),
            P(None, "grp", "tp", None),
            P(None, "grp", "tp"),
            P(None, "grp", None),
        ),
        check_vma=False,
    )
```

```python
import functools

import jax
import jax.numpy as jnp
from jax import lax
from jax.experimental import pallas as pl
from jax.experimental.pallas import tpu as pltpu
from jax.sharding import PartitionSpec as P

D = 2048
DH = 256
LAYERS = 2


epsilon = 1e-06


def from_partner(value, axis, apart):
    mask = 2**apart
    pairs = [(source, source ^ mask) for source in range(lax.axis_size(axis))]
    return lax.ppermute(value, axis, pairs)


def project(normed, weight):
    return lax.dot_general(
        normed, weight, (((1,), (1,)), ((), ())), preferred_element_type=jnp.float32
    )


def split_pieces(value):
    high = lax.optimization_barrier(value.astype(jnp.bfloat16))
    rest = value - high.astype(jnp.float32)
    middle = lax.optimization_barrier(rest.astype(jnp.bfloat16))
    lowest = (rest - middle.astype(jnp.float32)).astype(jnp.bfloat16)
    return jnp.stack([high, middle, lowest], axis=1)


def join_pieces(pieces):
    return jnp.sum(pieces.astype(jnp.float32), axis=-1)


def combine_halves(mine, theirs, lower):
    return jnp.where(
        lower, jnp.concatenate([mine, theirs], axis=1), jnp.concatenate([theirs, mine], axis=1)
    )


def one_cell(
    current,
    gain,
    w_query,
    w_key,
    w_value,
    w_outgate,
    w_gates,
    bias_forget,
    w_proj,
    cell,
    norm_vec,
    stab,
):
    heads = D // DH
    ncols = w_query.shape[0]
    group = DH // ncols
    device = lax.axis_index("tp")
    head = device // group
    cur_f = current.astype(jnp.float32)
    normed = (
        cur_f * lax.rsqrt(jnp.mean(cur_f * cur_f, axis=-1, keepdims=True) + epsilon) * gain
    ).astype(jnp.bfloat16)
    query = project(normed, w_query).astype(jnp.bfloat16)
    keys = (project(normed, w_key) * DH ** (-0.5)).astype(jnp.bfloat16)
    values = project(normed, w_value).astype(jnp.bfloat16)
    outgate = project(normed, w_outgate).astype(jnp.bfloat16)
    gates = jnp.dot(normed, w_gates, preferred_element_type=jnp.float32)
    in_gate = gates[:, :heads]
    log_forget = jax.nn.log_sigmoid(gates[:, heads:] + bias_forget)
    new_stab = jnp.maximum(log_forget + stab, in_gate)
    decay = jnp.exp(log_forget + stab - new_stab)
    weight_in = jnp.exp(in_gate - new_stab)
    select = (jnp.arange(heads) == head).astype(jnp.float32)
    my_decay = jnp.sum(decay * select, axis=-1)
    my_weight = jnp.sum(weight_in * select, axis=-1)
    my_stab = jnp.sum(new_stab * select, axis=-1)
    new_norm = my_decay[:, None] * norm_vec + my_weight[:, None] * keys.astype(jnp.float32)
    den_part = jnp.sum(query.astype(jnp.float32) * new_norm, axis=-1)
    q_head, k_head = (query, keys)
    denom = den_part
    for bit in range(group.bit_length() - 1):
        other_q, other_k, other_pieces = from_partner(
            (q_head, k_head, split_pieces(denom)), "tp", bit
        )
        lower = device // 2**bit % 2 == 0
        q_head = combine_halves(q_head, other_q, lower)
        k_head = combine_halves(k_head, other_k, lower)
        denom = denom + join_pieces(other_pieces)
    outer = values.astype(jnp.float32)[:, :, None] * k_head.astype(jnp.float32)[:, None, :]
    new_cell = my_decay[:, None, None] * cell + my_weight[:, None, None] * outer
    numer = jnp.einsum(
        "bk,bek->be", q_head.astype(jnp.float32), new_cell, precision=lax.Precision.HIGHEST
    )
    readout = numer / jnp.maximum(jnp.abs(denom), jnp.exp(-my_stab))[:, None]
    branch = (jax.nn.sigmoid(outgate.astype(jnp.float32)) * readout).astype(jnp.bfloat16)
    summed = project(lax.all_gather(branch, "tp", axis=1, tiled=True), w_proj)
    own_input = lax.dynamic_slice_in_dim(cur_f, device * ncols, ncols, 1)
    result = (own_input + summed).astype(jnp.bfloat16)
    return (result, new_cell, new_norm, new_stab)


def body(
    tokens,
    norm_gain,
    query_weight,
    key_weight,
    value_weight,
    outgate_weight,
    gate_weight,
    forget_bias,
    proj_weight,
    cell_state,
    normalizer,
    stabilizer,
):
    current = tokens
    cells = []
    norms = []
    stabs = []
    result = tokens
    for layer in range(LAYERS):
        result, new_cell, new_norm, new_stab = one_cell(
            current,
            norm_gain[layer],
            query_weight[layer],
            key_weight[layer],
            value_weight[layer],
            outgate_weight[layer],
            gate_weight[layer],
            forget_bias[layer],
            proj_weight[layer],
            cell_state[layer],
            normalizer[layer],
            stabilizer[layer],
        )
        cells.append(new_cell)
        norms.append(new_norm)
        stabs.append(new_stab)
        if layer + 1 < LAYERS:
            current = lax.all_gather(result, "tp", axis=1, tiled=True)
    return (result, jnp.stack(cells), jnp.stack(norms), jnp.stack(stabs))


NT = (((1,), (1,)), ((), ()))
CELL_CHUNKS = 4
MAIN_VMEM = 24 * 2**20
LAST_VMEM = 6 * 2**20


def flip(index, mask):
    result = index
    bit = 1
    while bit <= mask:
        if mask & bit:
            result = result + bit - 2 * bit * lax.rem(lax.div(index, bit), 2)
        bit *= 2
    return result


def sending_order(chips):
    return sorted(range(chips), key=lambda m: (-(m // 4), -(m % 2), -m))


def landing_order(chip, chips):
    ends = list(range(chips))
    inside = [0, 1] + list(range(chips - 1, 1, -1))
    place = lax.div(chip * 4, chips)
    inner = lax.rem(lax.div(place + 1, 2), 2)
    return [
        (
            flip(chip, a) + inner * (flip(chip, b) - flip(chip, a)),
            a + inner * (b - a),
            a,
        )
        for a, b in zip(ends, inside)
    ]


def fetch(source, target, sem):
    copy = pltpu.make_async_copy(source, target, sem)
    copy.start()
    return copy


def push(source, dest, target, send, recv):
    copy = pltpu.make_async_remote_copy(
        src_ref=source,
        dst_ref=dest,
        send_sem=send,
        recv_sem=recv,
        device_id={"tp": target},
        device_id_type=pl.DeviceIdType.MESH,
    )
    copy.start()
    return copy


def arrived(buffer, recv):
    pltpu.make_async_copy(buffer, buffer, recv).wait()


def greet_all(n, me):
    barrier = pltpu.get_barrier_semaphore()
    for i in range(1, n):
        pl.semaphore_signal(
            barrier,
            inc=1,
            device_id={"tp": lax.rem(me + i, n)},
            device_id_type=pl.DeviceIdType.MESH,
        )
    return barrier


def read_rows(cell_rows, queries, numer, start, rows):
    ncols = numer.shape[1]
    row = lax.broadcasted_iota(jnp.int32, (rows, ncols), 0)
    total = jnp.zeros((rows, ncols), jnp.float32)
    for b in range(rows):
        block = cell_rows(start + b).astype(jnp.bfloat16)
        product = lax.dot_general(queries, block, NT, preferred_element_type=jnp.float32)
        total = jnp.where(row == b, product, total)
    numer[pl.ds(start, rows), :] = total


def head_sums(q_head, k_head, n_head, my_stab, my_decay, my_weight):
    denom = jnp.sum(q_head * (my_decay * n_head + my_weight * k_head), axis=-1, keepdims=True)
    inner = jnp.sum(q_head * k_head, axis=-1, keepdims=True)
    return inner, jnp.maximum(jnp.abs(denom), jnp.exp(-my_stab))


def send_half(half, chip, core, chips, rows, source, dest, send, recv):
    me = chip * 2 + core
    return [
        push(
            source.at[pl.ds(half * rows, rows)],
            dest.at[me],
            flip(chip, m) * 2 + half,
            send.at[half, m],
            recv.at[m, core],
        )
        for m in sending_order(chips)
        if m
    ]


def send_across(chip, core, rows, source, dest, send, recv):
    me = chip * 2 + core
    dest[me] = source[pl.ds(pl.multiple_of(core * rows, rows), rows), :]
    return push(
        source.at[pl.ds(pl.multiple_of((1 - core) * rows, rows), rows)],
        dest.at[me],
        chip * 2 + 1 - core,
        send.at[0, 0],
        recv.at[0, core],
    )


def gather_project(chip, core, chips, rows, dest, recv, weights):
    partner = chip * 2 + 1 - core
    ncols = dest.shape[2]
    total = jnp.zeros((rows, 2 * ncols), jnp.float32)
    for other, m, at in landing_order(chip, chips):
        if at == 0:
            arrived(dest.at[partner], recv.at[0, 1 - core])
        else:
            for c in range(2):
                arrived(dest.at[other * 2 + c], recv.at[m, c])
        block = jnp.concatenate([dest[other * 2], dest[other * 2 + 1]], axis=1)
        part = weights[:, pl.ds(pl.multiple_of(other * 2 * ncols, 2 * ncols), 2 * ncols)]
        total = total + lax.dot_general(block, part, NT, preferred_element_type=jnp.float32)
    return total


def cells_kernel(
    n,
    tokens,
    norm_gain,
    w_query,
    w_key,
    w_value,
    w_outgate,
    w_gates,
    bias_forget,
    w_proj,
    cell,
    norm_vec,
    stab,
    cell_buf,
    new_norm,
    new_stab,
    wv_buf,
    key_buf,
    decay_buf,
    q_out,
    norm_out,
    scale_out,
    gate_out,
    own_out,
    proj_out,
    tok_buf,
    gain_buf,
    weights,
    wide,
    proj_buf,
    gate_buf,
    bias_buf,
    stab_buf,
    norm_buf,
    pair_buf,
    send_buf,
    branch_buf,
    result_buf,
    result_out,
    whole_buf,
    swap_buf,
    swap_out,
    gates_buf,
    numer_buf,
    small_sem,
    weight_sem,
    wide_sem,
    cell_sem,
    pair_send,
    pair_recv,
    branch_send,
    branch_recv,
    result_send,
    result_recv,
):
    layers, batch, ncols, dh = cell.shape
    width = tokens.shape[1]
    heads = stab.shape[1]
    rows = batch // CELL_CHUNKS
    half = batch // 2
    chips = n // 2
    me = lax.axis_index("tp")
    core = lax.rem(me, 2)
    chip = lax.div(me, 2)
    partner = chip * 2 + 1 - core
    barrier = greet_all(n, me)

    tok_copy = fetch(tokens, tok_buf, small_sem.at[0])
    gain_copy = fetch(norm_gain, gain_buf, small_sem.at[1])
    names = [w_query, w_key, w_value, w_outgate]
    weight_copies = [
        fetch(names[i].at[0], weights.at[pl.ds(i * ncols, ncols)], weight_sem.at[i])
        for i in range(4)
    ]
    small = [
        fetch(w_gates, gate_buf, small_sem.at[2]),
        fetch(bias_forget, bias_buf, small_sem.at[3]),
        fetch(stab, stab_buf, small_sem.at[4]),
    ]
    norm_copy = fetch(norm_vec, norm_buf.at[core], small_sem.at[5])

    def fetch_cell(layer):
        return [
            fetch(
                cell.at[layer, pl.ds(c * rows, rows)],
                cell_buf.at[layer, pl.ds(c * rows, rows)],
                cell_sem.at[layer, c],
            )
            for c in range(CELL_CHUNKS)
        ]

    def own_rows(ref, i):
        return ref.at[pl.ds(pl.multiple_of(i * 2 * ncols + core * ncols, ncols), ncols)]

    def scale(gates, layer, old_stab):
        in_gate = gates[:, :heads]
        forget = gates[:, heads : 2 * heads] + bias_buf[pl.ds(layer, 1), :]
        log_forget = jnp.minimum(forget, 0.0) - jnp.log1p(jnp.exp(-jnp.abs(forget)))
        next_stab = jnp.maximum(log_forget + old_stab, in_gate)
        mine = lax.broadcasted_iota(jnp.int32, next_stab.shape, 1) == chip

        def pick(entry):
            return jnp.sum(jnp.where(mine, entry, 0.0), axis=-1, keepdims=True)

        my_stab = pick(next_stab)
        my_decay = jnp.exp(pick(log_forget + old_stab) - my_stab)
        my_weight = jnp.exp(pick(in_gate) - my_stab)
        return next_stab, my_stab, my_decay, my_weight

    gain_copy.wait()
    tok_copy.wait()
    cell_copies = fetch_cell(0)
    proj_copies = [fetch(w_proj.at[0], own_rows(proj_buf, 0), small_sem.at[6])]
    wide_copies = [
        fetch(names[i].at[1], own_rows(wide, i), wide_sem.at[i]) for i in range(4)
    ]
    current = tok_buf[...].astype(jnp.float32)
    mean = jnp.sum(current * current, axis=-1, keepdims=True) * (1.0 / width)
    normed = (current * lax.rsqrt(mean + epsilon) * gain_buf[0:1, :]).astype(jnp.bfloat16)
    weight_copies[0].wait()
    weight_copies[1].wait()
    both = lax.dot_general(
        normed, weights[: 2 * ncols], NT, preferred_element_type=jnp.float32
    )
    pair_buf[core, 0] = both[:, :ncols].astype(jnp.bfloat16)
    key = (both[:, ncols:] * dh ** (-0.5)).astype(jnp.bfloat16)
    pair_buf[core, 1] = key
    weight_copies[2].wait()
    weight_copies[3].wait()
    for copy in small:
        copy.wait()
    norm_copy.wait()
    pl.semaphore_wait(barrier, n - 1)
    pair_copies = [
        push(pair_buf.at[core], pair_buf.at[core], partner, pair_send.at[0], pair_recv.at[0]),
        push(norm_buf.at[core], norm_buf.at[core], partner, pair_send.at[1], pair_recv.at[1]),
    ]
    both = lax.dot_general(
        normed, weights[2 * ncols :], NT, preferred_element_type=jnp.float32
    )
    value = both[:, :ncols].astype(jnp.bfloat16).astype(jnp.float32)
    gate = jax.nn.sigmoid(both[:, ncols:].astype(jnp.bfloat16).astype(jnp.float32))
    gates = lax.dot_general(normed, gate_buf[0], NT, preferred_element_type=jnp.float32)
    next_stab, my_stab, my_decay, my_weight = scale(gates, 0, stab_buf[0].T)
    new_stab[0] = next_stab.T
    new_norm[0] = my_decay * norm_buf[core, 0] + my_weight * key.astype(jnp.float32)
    weighted = my_weight * value
    wv_buf[0] = weighted
    decay_buf[0] = jnp.broadcast_to(my_decay, (batch, ncols))
    arrived(pair_buf.at[1 - core], pair_recv.at[0])
    arrived(norm_buf.at[1 - core], pair_recv.at[1])
    q_head = jnp.concatenate([pair_buf[j, 0] for j in range(2)], axis=1).astype(jnp.float32)
    k_head = jnp.concatenate([pair_buf[j, 1] for j in range(2)], axis=1).astype(jnp.float32)
    key_buf[0] = k_head
    n_head = jnp.concatenate([norm_buf[j, 0] for j in range(2)], axis=1)
    inner, den = head_sums(q_head, k_head, n_head, my_stab, my_decay, my_weight)

    branch_copies = []
    for h in range(2):
        for c in range(h * CELL_CHUNKS // 2, (h + 1) * CELL_CHUNKS // 2):
            cell_copies[c].wait()
        for c in range(h * CELL_CHUNKS // 2, (h + 1) * CELL_CHUNKS // 2):
            queries = jnp.concatenate(
                [pair_buf[j, 0, pl.ds(c * rows, rows), :] for j in range(2)], axis=1
            )
            read_rows(lambda b: cell_buf[0, b], queries, numer_buf, c * rows, rows)
        part = slice(h * half, (h + 1) * half)
        numer = my_decay[part] * numer_buf[part, :] + weighted[part] * inner[part]
        send_buf[part, :] = (gate[part] * (numer / den[part])).astype(jnp.bfloat16)
        branch_copies += send_half(
            h, chip, core, chips, half, send_buf, branch_buf, branch_send, branch_recv
        )
    branch_copies.append(
        send_across(chip, core, half, send_buf, branch_buf, branch_send, branch_recv)
    )
    proj_copies[0].wait()
    pair_copies.append(
        push(own_rows(proj_buf, 0), own_rows(proj_buf, 0), partner, pair_send.at[2], pair_recv.at[2])
    )
    wide_pushes = []
    for i in range(4):
        wide_copies[i].wait()
        wide_pushes.append(
            push(
                own_rows(wide, i),
                own_rows(wide, i),
                partner,
                pair_send.at[3 + i],
                pair_recv.at[3 + i],
            )
        )
    proj_copies.append(fetch(w_proj.at[1], own_rows(proj_out, 0), small_sem.at[7]))
    cell_copies = fetch_cell(1)
    arrived(
        proj_buf.at[pl.ds(pl.multiple_of((1 - core) * ncols, ncols), ncols)], pair_recv.at[2]
    )
    summed = gather_project(chip, core, chips, half, branch_buf, branch_recv, proj_buf)
    my_rows = pl.ds(pl.multiple_of(core * half, half), half)
    my_cols = pl.ds(pl.multiple_of(chip * 2 * ncols, 2 * ncols), 2 * ncols)
    result = (tok_buf[my_rows, my_cols].astype(jnp.float32) + summed).astype(jnp.bfloat16)
    own_out[...] = result
    result_out[...] = result
    result_copies = [
        push(
            result_out,
            result_buf.at[chip],
            flip(chip, m) * 2 + 1 - core,
            result_send.at[m],
            result_recv.at[m],
        )
        for m in sending_order(chips)
    ]
    proj_copies[1].wait()
    pair_copies.append(
        push(own_rows(proj_out, 0), own_rows(proj_out, 0), partner, pair_send.at[9], pair_recv.at[9])
    )

    for i in range(4):
        arrived(
            wide.at[pl.ds(pl.multiple_of(i * 2 * ncols + (1 - core) * ncols, ncols), ncols)],
            pair_recv.at[3 + i],
        )
    total = jnp.zeros((half, 8 * ncols), jnp.float32)
    gates = jnp.zeros((half, 2 * heads), jnp.float32)
    square = jnp.zeros((half, 1), jnp.float32)
    for other, m, _ in landing_order(chip, chips):
        arrived(result_buf.at[other], result_recv.at[m])
        cols = pl.ds(pl.multiple_of(other * 2 * ncols, 2 * ncols), 2 * ncols)
        block = result_buf[other].astype(jnp.float32)
        square = square + jnp.sum(block * block, axis=-1, keepdims=True)
        block = (block * gain_buf[1:2, cols]).astype(jnp.bfloat16)
        total = total + lax.dot_general(
            block, wide[:, cols], NT, preferred_element_type=jnp.float32
        )
        gates = gates + lax.dot_general(
            block, gate_buf[1, :, cols], NT, preferred_element_type=jnp.float32
        )
    root = lax.rsqrt(square * (1.0 / width) + epsilon)
    old_stab = jnp.where(core == 0, stab_buf[1].T[half:], stab_buf[1].T[:half])
    scalars = scale(gates * root, 1, old_stab)
    gates_buf[1 - core] = jnp.concatenate(
        scalars + (jnp.zeros((half, ncols - heads - 3), jnp.float32),), axis=1
    )
    total = total * root
    query = total[:, : 2 * ncols].astype(jnp.bfloat16)
    key = (total[:, 2 * ncols : 4 * ncols] * dh ** (-0.5)).astype(jnp.bfloat16)
    whole_buf[...] = total[:, 4 * ncols :].astype(jnp.bfloat16)
    for target, side in ((swap_out, 1 - core), (swap_buf.at[1 - core], core)):
        target[:, : 2 * ncols] = query
        target[:, 2 * ncols : 4 * ncols] = key
        for i in range(2):
            target[:, (4 + i) * ncols : (5 + i) * ncols] = whole_buf[
                :, pl.ds(pl.multiple_of(i * 2 * ncols + side * ncols, ncols), ncols)
            ]
    pair_copies += [
        push(swap_out, swap_buf.at[1 - core], partner, pair_send.at[7], pair_recv.at[7]),
        push(
            gates_buf.at[1 - core],
            gates_buf.at[1 - core],
            partner,
            pair_send.at[8],
            pair_recv.at[8],
        ),
    ]
    for j in range(2):
        norm_out[j] = norm_buf[j, 1]
    for copy in branch_copies + wide_pushes + result_copies:
        copy.wait_send()
    for copy in cell_copies:
        copy.wait()
    arrived(
        proj_out.at[pl.ds(pl.multiple_of((1 - core) * ncols, ncols), ncols)], pair_recv.at[9]
    )
    arrived(swap_buf.at[core], pair_recv.at[7])
    arrived(gates_buf.at[core], pair_recv.at[8])

    def both_halves(part):
        return jnp.concatenate([swap_buf[j, :, part] for j in range(2)], axis=0)

    scalars = jnp.concatenate([gates_buf[j] for j in range(2)], axis=0)
    scale_out[...] = scalars
    new_stab[1] = scalars[:, :heads].T
    my_decay = scalars[:, heads + 1 : heads + 2]
    my_weight = scalars[:, heads + 2 : heads + 3]
    q_out[...] = both_halves(slice(0, 2 * ncols))
    key_buf[1] = both_halves(slice(2 * ncols, 4 * ncols)).astype(jnp.float32)
    wv_buf[1] = my_weight * both_halves(slice(4 * ncols, 5 * ncols)).astype(jnp.float32)
    decay_buf[1] = jnp.broadcast_to(my_decay, (batch, ncols))
    gate_out[...] = both_halves(slice(5 * ncols, 6 * ncols))
    key = both_halves(pl.ds(pl.multiple_of((2 + core) * ncols, ncols), ncols))
    new_norm[1] = my_decay * norm_buf[core, 1] + my_weight * key.astype(jnp.float32)
    for copy in pair_copies:
        copy.wait_send()


def last_kernel(
    n,
    heads,
    cell_buf,
    queries,
    keys,
    norms,
    weighted,
    scalars,
    outgate,
    own,
    proj_buf,
    _,
    mixed,
    send_buf,
    branch_buf,
    swap_buf,
    swap_out,
    numer_buf,
    pair_send,
    pair_recv,
    branch_send,
    branch_recv,
):
    layers, batch, ncols, dh = cell_buf.shape
    last = layers - 1
    rows = batch // CELL_CHUNKS
    half = batch // 2
    chips = n // 2
    me = lax.axis_index("tp")
    core = lax.rem(me, 2)
    chip = lax.div(me, 2)
    partner = chip * 2 + 1 - core
    barrier = greet_all(n, me)
    for c in range(CELL_CHUNKS):
        read_rows(
            lambda b: cell_buf[last, b],
            queries[pl.ds(c * rows, rows), :],
            numer_buf,
            c * rows,
            rows,
        )
    q_head = queries[...].astype(jnp.float32)
    n_head = jnp.concatenate([norms[j] for j in range(2)], axis=1)
    my_stab, my_decay, my_weight = (scalars[:, heads + i : heads + i + 1] for i in range(3))
    inner, den = head_sums(q_head, keys[last], n_head, my_stab, my_decay, my_weight)
    numer = my_decay * numer_buf[...] + weighted[last] * inner
    gate = jax.nn.sigmoid(outgate[...].astype(jnp.float32))
    send_buf[...] = (gate * (numer / den)).astype(jnp.bfloat16)
    pl.semaphore_wait(barrier, n - 1)
    copies = []
    for h in range(2):
        copies += send_half(
            h, chip, core, chips, half, send_buf, branch_buf, branch_send, branch_recv
        )
    copies.append(send_across(chip, core, half, send_buf, branch_buf, branch_send, branch_recv))
    summed = gather_project(chip, core, chips, half, branch_buf, branch_recv, proj_buf)
    result = (own[...].astype(jnp.float32) + summed).astype(jnp.bfloat16)
    swap_buf[...] = result
    swap_out[core] = swap_buf[:, pl.ds(pl.multiple_of((1 - core) * ncols, ncols), ncols)]
    swap_copy = push(swap_out.at[core], swap_out.at[2 + core], partner, pair_send, pair_recv)
    mixed[pl.ds(pl.multiple_of(core * half, half), half), :] = swap_buf[
        :, pl.ds(pl.multiple_of(core * ncols, ncols), ncols)
    ]
    for copy in copies:
        copy.wait_send()
    arrived(swap_out.at[3 - core], pair_recv)
    mixed[pl.ds(pl.multiple_of((1 - core) * half, half), half), :] = swap_out[3 - core]
    swap_copy.wait_send()


def fused_body(n, *args):
    (tokens, norm_gain, w_query, _, _, _, w_gates, bias_forget, _, cell, norm_vec, stab) = args
    layers, batch, ncols, dh = cell.shape
    width = tokens.shape[1]
    half = batch // 2
    chips = n // 2
    w_gates = jnp.swapaxes(w_gates, 1, 2)
    stab = jnp.swapaxes(stab, 1, 2)
    args = args[:6] + (w_gates,) + args[7:11] + (stab,)
    args = [pltpu.with_memory_space_constraint(arg, pltpu.HBM) for arg in args]
    bf16, f32 = jnp.bfloat16, jnp.float32
    vmem = pl.BlockSpec(memory_space=pltpu.VMEM)
    hbm = pl.BlockSpec(memory_space=pltpu.HBM)
    dma = pltpu.SemaphoreType.DMA
    held, new_norm, new_stab, weighted, keys, decay, *rest = pl.pallas_call(
        functools.partial(cells_kernel, n),
        out_shape=(
            pltpu.VMEM(cell.shape, f32),
            jax.ShapeDtypeStruct(norm_vec.shape, f32),
            jax.ShapeDtypeStruct(stab.shape, f32),
            jax.ShapeDtypeStruct((layers, batch, ncols), f32),
            jax.ShapeDtypeStruct((layers, batch, dh), f32),
            jax.ShapeDtypeStruct((layers, batch, ncols), f32),
            jax.ShapeDtypeStruct((batch, dh), bf16),
            jax.ShapeDtypeStruct((2, batch, ncols), f32),
            jax.ShapeDtypeStruct((batch, ncols), f32),
            jax.ShapeDtypeStruct((batch, ncols), bf16),
            jax.ShapeDtypeStruct((half, dh), bf16),
            jax.ShapeDtypeStruct((2 * ncols, width), bf16),
        ),
        in_specs=[hbm] * len(args),
        out_specs=(vmem,) * 12,
        scratch_shapes=[
            pltpu.VMEM(tokens.shape, bf16),
            pltpu.VMEM(norm_gain.shape, f32),
            pltpu.VMEM((4 * ncols, width), bf16),
            pltpu.VMEM((8 * ncols, width), bf16),
            pltpu.VMEM((2 * ncols, width), bf16),
            pltpu.VMEM(w_gates.shape, bf16),
            pltpu.VMEM(bias_forget.shape, f32),
            pltpu.VMEM(stab.shape, f32),
            pltpu.VMEM((2,) + norm_vec.shape, f32),
            pltpu.VMEM((2, 2, batch, ncols), bf16),
            pltpu.VMEM((batch, ncols), bf16),
            pltpu.VMEM((n, half, ncols), bf16),
            pltpu.VMEM((chips, half, 2 * ncols), bf16),
            pltpu.VMEM((half, 2 * ncols), bf16),
            pltpu.VMEM((half, 4 * ncols), bf16),
            pltpu.VMEM((2, half, 6 * ncols), bf16),
            pltpu.VMEM((half, 6 * ncols), bf16),
            pltpu.VMEM((2, half, ncols), f32),
            pltpu.VMEM((batch, ncols), f32),
            dma((8,)),
            dma((4,)),
            dma((4,)),
            dma((layers, CELL_CHUNKS)),
            dma((10,)),
            dma((10,)),
            dma((2, chips)),
            dma((chips, 2)),
            dma((chips,)),
            dma((chips,)),
        ],
        compiler_params=pltpu.CompilerParams(
            collective_id=0, has_side_effects=True, vmem_limit_bytes=MAIN_VMEM
        ),
        name="cells",
    )(*args)
    new_cell = (
        decay[:, :, :1, None] * held + weighted[:, :, :, None] * keys[:, :, None, :]
    )
    queries, norms, scalars, outgate, own, proj = rest
    mixed = pl.pallas_call(
        functools.partial(last_kernel, n, stab.shape[1]),
        out_shape=jax.ShapeDtypeStruct((batch, ncols), bf16),
        in_specs=[vmem] * 10,
        out_specs=vmem,
        scratch_shapes=[
            pltpu.VMEM((batch, ncols), bf16),
            pltpu.VMEM((n, half, ncols), bf16),
            pltpu.VMEM((half, 2 * ncols), bf16),
            pltpu.VMEM((4, half, ncols), bf16),
            pltpu.VMEM((batch, ncols), f32),
            dma,
            dma,
            dma((2, chips)),
            dma((chips, 2)),
        ],
        compiler_params=pltpu.CompilerParams(
            collective_id=1, has_side_effects=True, vmem_limit_bytes=LAST_VMEM
        ),
        cost_estimate=pl.CostEstimate(
            flops=5 * 10**10, bytes_accessed=10**6, transcendentals=0
        ),
        name="last",
    )(
        held,
        queries,
        keys,
        norms,
        weighted,
        scalars,
        outgate,
        own,
        proj,
        new_cell[0, 0, :8, :128],
    )
    mixed, new_norm, new_stab = write_small(mixed, new_norm, new_stab)
    return mixed, new_cell, new_norm, jnp.swapaxes(new_stab, 1, 2)


def write_kernel(*refs):
    half = len(refs) // 2
    sems = refs[-1]
    copies = [
        pltpu.make_async_copy(refs[i], refs[half + i], sems.at[i]) for i in range(half)
    ]
    for copy in copies:
        copy.start()
    for copy in copies:
        copy.wait()


def write_small(*arrays):
    return pl.pallas_call(
        write_kernel,
        out_shape=[jax.ShapeDtypeStruct(x.shape, x.dtype) for x in arrays],
        in_specs=[pl.BlockSpec(memory_space=pltpu.VMEM)] * len(arrays),
        out_specs=[pl.BlockSpec(memory_space=pltpu.HBM)] * len(arrays),
        scratch_shapes=[pltpu.SemaphoreType.DMA((len(arrays),))],
        compiler_params=pltpu.CompilerParams(vmem_limit_bytes=2**20),
        name="write",
    )(*arrays)


def whole_body(*args):
    n = lax.axis_size("tp")
    layers, batch, ncols, dh = args[9].shape
    heads = args[11].shape[2]
    if (
        layers == 2
        and n == 2 * heads
        and n & (n - 1) == 0
        and ncols % 128 == 0
        and dh == 2 * ncols
        and batch % (16 * CELL_CHUNKS) == 0
    ):
        return fused_body(n, *args)
    return body(*args)


def solution(mesh):
    return jax.shard_map(
        whole_body,
        mesh=mesh,
        in_specs=(
            P("grp", None),
            P(),
            P(None, "tp", None),
            P(None, "tp", None),
            P(None, "tp", None),
            P(None, "tp", None),
            P(),
            P(),
            P(None, "tp", None),
            P(None, "grp", "tp", None),
            P(None, "grp", "tp"),
            P(None, "grp", None),
        ),
        out_specs=(
            P("grp", "tp"),
            P(None, "grp", "tp", None),
            P(None, "grp", "tp"),
            P(None, "grp", None),
        ),
        check_vma=False,
    )
```

```python
import functools

import jax
import jax.numpy as jnp
from jax import lax
from jax.experimental import pallas as pl
from jax.experimental.pallas import tpu as pltpu
from jax.sharding import PartitionSpec as P

D = 2048
DH = 256
LAYERS = 2


epsilon = 1e-06


def from_partner(value, axis, apart):
    mask = 2**apart
    pairs = [(source, source ^ mask) for source in range(lax.axis_size(axis))]
    return lax.ppermute(value, axis, pairs)


def project(normed, weight):
    return lax.dot_general(
        normed, weight, (((1,), (1,)), ((), ())), preferred_element_type=jnp.float32
    )


def split_pieces(value):
    high = lax.optimization_barrier(value.astype(jnp.bfloat16))
    rest = value - high.astype(jnp.float32)
    middle = lax.optimization_barrier(rest.astype(jnp.bfloat16))
    lowest = (rest - middle.astype(jnp.float32)).astype(jnp.bfloat16)
    return jnp.stack([high, middle, lowest], axis=1)


def join_pieces(pieces):
    return jnp.sum(pieces.astype(jnp.float32), axis=-1)


def combine_halves(mine, theirs, lower):
    return jnp.where(
        lower, jnp.concatenate([mine, theirs], axis=1), jnp.concatenate([theirs, mine], axis=1)
    )


def one_cell(
    current,
    gain,
    w_query,
    w_key,
    w_value,
    w_outgate,
    w_gates,
    bias_forget,
    w_proj,
    cell,
    norm_vec,
    stab,
):
    heads = D // DH
    ncols = w_query.shape[0]
    group = DH // ncols
    device = lax.axis_index("tp")
    head = device // group
    cur_f = current.astype(jnp.float32)
    normed = (
        cur_f * lax.rsqrt(jnp.mean(cur_f * cur_f, axis=-1, keepdims=True) + epsilon) * gain
    ).astype(jnp.bfloat16)
    query = project(normed, w_query).astype(jnp.bfloat16)
    keys = (project(normed, w_key) * DH ** (-0.5)).astype(jnp.bfloat16)
    values = project(normed, w_value).astype(jnp.bfloat16)
    outgate = project(normed, w_outgate).astype(jnp.bfloat16)
    gates = jnp.dot(normed, w_gates, preferred_element_type=jnp.float32)
    in_gate = gates[:, :heads]
    log_forget = jax.nn.log_sigmoid(gates[:, heads:] + bias_forget)
    new_stab = jnp.maximum(log_forget + stab, in_gate)
    decay = jnp.exp(log_forget + stab - new_stab)
    weight_in = jnp.exp(in_gate - new_stab)
    select = (jnp.arange(heads) == head).astype(jnp.float32)
    my_decay = jnp.sum(decay * select, axis=-1)
    my_weight = jnp.sum(weight_in * select, axis=-1)
    my_stab = jnp.sum(new_stab * select, axis=-1)
    new_norm = my_decay[:, None] * norm_vec + my_weight[:, None] * keys.astype(jnp.float32)
    den_part = jnp.sum(query.astype(jnp.float32) * new_norm, axis=-1)
    q_head, k_head = (query, keys)
    denom = den_part
    for bit in range(group.bit_length() - 1):
        other_q, other_k, other_pieces = from_partner(
            (q_head, k_head, split_pieces(denom)), "tp", bit
        )
        lower = device // 2**bit % 2 == 0
        q_head = combine_halves(q_head, other_q, lower)
        k_head = combine_halves(k_head, other_k, lower)
        denom = denom + join_pieces(other_pieces)
    outer = values.astype(jnp.float32)[:, :, None] * k_head.astype(jnp.float32)[:, None, :]
    new_cell = my_decay[:, None, None] * cell + my_weight[:, None, None] * outer
    numer = jnp.einsum(
        "bk,bek->be", q_head.astype(jnp.float32), new_cell, precision=lax.Precision.HIGHEST
    )
    readout = numer / jnp.maximum(jnp.abs(denom), jnp.exp(-my_stab))[:, None]
    branch = (jax.nn.sigmoid(outgate.astype(jnp.float32)) * readout).astype(jnp.bfloat16)
    summed = project(lax.all_gather(branch, "tp", axis=1, tiled=True), w_proj)
    own_input = lax.dynamic_slice_in_dim(cur_f, device * ncols, ncols, 1)
    result = (own_input + summed).astype(jnp.bfloat16)
    return (result, new_cell, new_norm, new_stab)


def body(
    tokens,
    norm_gain,
    query_weight,
    key_weight,
    value_weight,
    outgate_weight,
    gate_weight,
    forget_bias,
    proj_weight,
    cell_state,
    normalizer,
    stabilizer,
):
    current = tokens
    cells = []
    norms = []
    stabs = []
    result = tokens
    for layer in range(LAYERS):
        result, new_cell, new_norm, new_stab = one_cell(
            current,
            norm_gain[layer],
            query_weight[layer],
            key_weight[layer],
            value_weight[layer],
            outgate_weight[layer],
            gate_weight[layer],
            forget_bias[layer],
            proj_weight[layer],
            cell_state[layer],
            normalizer[layer],
            stabilizer[layer],
        )
        cells.append(new_cell)
        norms.append(new_norm)
        stabs.append(new_stab)
        if layer + 1 < LAYERS:
            current = lax.all_gather(result, "tp", axis=1, tiled=True)
    return (result, jnp.stack(cells), jnp.stack(norms), jnp.stack(stabs))


NT = (((1,), (1,)), ((), ()))
CELL_CHUNKS = 4
MAIN_VMEM = 24 * 2**20
LAST_VMEM = 6 * 2**20


def flip(index, mask):
    result = index
    bit = 1
    while bit <= mask:
        if mask & bit:
            result = result + bit - 2 * bit * lax.rem(lax.div(index, bit), 2)
        bit *= 2
    return result


def sending_order(chips):
    return sorted(range(chips), key=lambda m: (-(m // 4), -(m % 2), -m))


def first_to_zero(chip, chips):
    masks = [m for m in sending_order(chips) if m]
    pairs = []
    for at, m in enumerate(masks):
        same = 1 - lax.div((chip - m) * (chip - m) + chips * chips - 1, chips * chips)
        if at == 0:
            zero = 1 - lax.div(chip * chip + chips * chips - 1, chips * chips)
            pairs.append((zero * flip(chip, m), chip + zero * m))
        else:
            top = masks[0]
            pairs.append(
                (flip(chip, m) + same * (flip(chip, top) - flip(chip, m)), m + same * (top - m))
            )
    return pairs


def landing_order(chip, chips):
    ends = list(range(chips))
    inside = [0, 1] + list(range(chips - 1, 1, -1))
    place = lax.div(chip * 4, chips)
    inner = lax.rem(lax.div(place + 1, 2), 2)
    return [
        (
            flip(chip, a) + inner * (flip(chip, b) - flip(chip, a)),
            a + inner * (b - a),
            a,
        )
        for a, b in zip(ends, inside)
    ]


def fetch(source, target, sem):
    copy = pltpu.make_async_copy(source, target, sem)
    copy.start()
    return copy


def push(source, dest, target, send, recv):
    copy = pltpu.make_async_remote_copy(
        src_ref=source,
        dst_ref=dest,
        send_sem=send,
        recv_sem=recv,
        device_id={"tp": target},
        device_id_type=pl.DeviceIdType.MESH,
    )
    copy.start()
    return copy


def arrived(buffer, recv):
    pltpu.make_async_copy(buffer, buffer, recv).wait()


def greet_all(n, me):
    barrier = pltpu.get_barrier_semaphore()
    for i in range(1, n):
        pl.semaphore_signal(
            barrier,
            inc=1,
            device_id={"tp": lax.rem(me + i, n)},
            device_id_type=pl.DeviceIdType.MESH,
        )
    return barrier


def read_rows(cell_rows, queries, numer, start, rows):
    ncols = numer.shape[1]
    row = lax.broadcasted_iota(jnp.int32, (rows, ncols), 0)
    total = jnp.zeros((rows, ncols), jnp.float32)
    for b in range(rows):
        block = cell_rows(start + b).astype(jnp.bfloat16)
        product = lax.dot_general(queries, block, NT, preferred_element_type=jnp.float32)
        total = jnp.where(row == b, product, total)
    numer[pl.ds(start, rows), :] = total


def update_rows(cells, decay, weighted, keys):
    columns = weighted.T
    for r in range(weighted.shape[0]):
        row = slice(r, r + 1)
        cells[r] = decay[row] * cells[r] + columns[:, row] * keys[row]


def bound(q_head, k_head, n_head, my_stab, my_decay, my_weight):
    denom = jnp.sum(q_head * (my_decay * n_head + my_weight * k_head), axis=-1, keepdims=True)
    return jnp.maximum(jnp.abs(denom), jnp.exp(-my_stab))


def send_half(half, chip, core, chips, rows, source, dest, send, recv):
    me = chip * 2 + core
    return [
        push(
            source.at[pl.ds(half * rows, rows)],
            dest.at[me],
            flip(chip, m) * 2 + half,
            send.at[half, m],
            recv.at[m, core],
        )
        for m in sending_order(chips)
        if m
    ]


def send_across(chip, core, rows, source, dest, send, recv):
    me = chip * 2 + core
    dest[me] = source[pl.ds(pl.multiple_of(core * rows, rows), rows), :]
    return push(
        source.at[pl.ds(pl.multiple_of((1 - core) * rows, rows), rows)],
        dest.at[me],
        chip * 2 + 1 - core,
        send.at[0, 0],
        recv.at[0, core],
    )


def gather_project(chip, core, chips, rows, dest, recv, weights):
    partner = chip * 2 + 1 - core
    ncols = dest.shape[2]
    total = jnp.zeros((rows, 2 * ncols), jnp.float32)
    for other, m, at in landing_order(chip, chips):
        if at == 0:
            arrived(dest.at[partner], recv.at[0, 1 - core])
        else:
            for c in range(2):
                arrived(dest.at[other * 2 + c], recv.at[m, c])
        block = jnp.concatenate([dest[other * 2], dest[other * 2 + 1]], axis=1)
        part = weights[:, pl.ds(pl.multiple_of(other * 2 * ncols, 2 * ncols), 2 * ncols)]
        total = total + lax.dot_general(block, part, NT, preferred_element_type=jnp.float32)
    return total


def cells_kernel(
    n,
    tokens,
    norm_gain,
    w_query,
    w_key,
    w_value,
    w_outgate,
    w_gates,
    bias_forget,
    w_proj,
    cell,
    norm_vec,
    stab,
    cell_buf,
    new_norm,
    new_stab,
    one_out,
    key_out,
    q_out,
    norm_out,
    scale_out,
    gate_out,
    own_out,
    proj_out,
    tok_buf,
    gain_buf,
    weights,
    wide,
    proj_buf,
    gate_buf,
    bias_buf,
    stab_buf,
    norm_buf,
    pair_buf,
    send_buf,
    branch_buf,
    result_buf,
    result_out,
    whole_buf,
    swap_buf,
    swap_out,
    gates_buf,
    numer_buf,
    small_sem,
    weight_sem,
    wide_sem,
    cell_sem,
    pair_send,
    pair_recv,
    branch_send,
    branch_recv,
    result_send,
    result_recv,
):
    layers, batch, ncols, dh = cell.shape
    width = tokens.shape[1]
    heads = stab.shape[1]
    rows = batch // CELL_CHUNKS
    half = batch // 2
    chips = n // 2
    me = lax.axis_index("tp")
    core = lax.rem(me, 2)
    chip = lax.div(me, 2)
    partner = chip * 2 + 1 - core
    barrier = greet_all(n, me)

    tok_copy = fetch(tokens, tok_buf, small_sem.at[0])
    gain_copy = fetch(norm_gain, gain_buf, small_sem.at[1])
    names = [w_query, w_key, w_value, w_outgate]
    weight_copies = [
        fetch(names[i].at[0], weights.at[pl.ds(i * ncols, ncols)], weight_sem.at[i])
        for i in range(4)
    ]
    small = [
        fetch(w_gates, gate_buf, small_sem.at[2]),
        fetch(bias_forget, bias_buf, small_sem.at[3]),
        fetch(stab, stab_buf, small_sem.at[4]),
    ]
    norm_copy = fetch(norm_vec, norm_buf.at[core], small_sem.at[5])

    def fetch_cell(layer):
        return [
            fetch(
                cell.at[layer, pl.ds(c * rows, rows)],
                cell_buf.at[layer, pl.ds(c * rows, rows)],
                cell_sem.at[layer, c],
            )
            for c in range(CELL_CHUNKS)
        ]

    def own_rows(ref, i):
        return ref.at[pl.ds(pl.multiple_of(i * 2 * ncols + core * ncols, ncols), ncols)]

    def scale(gates, layer, old_stab):
        in_gate = gates[:, :heads]
        forget = gates[:, heads : 2 * heads] + bias_buf[pl.ds(layer, 1), :]
        log_forget = jnp.minimum(forget, 0.0) - jnp.log1p(jnp.exp(-jnp.abs(forget)))
        next_stab = jnp.maximum(log_forget + old_stab, in_gate)
        mine = lax.broadcasted_iota(jnp.int32, next_stab.shape, 1) == chip

        def pick(entry):
            return jnp.sum(jnp.where(mine, entry, 0.0), axis=-1, keepdims=True)

        my_stab = pick(next_stab)
        my_decay = jnp.exp(pick(log_forget + old_stab) - my_stab)
        my_weight = jnp.exp(pick(in_gate) - my_stab)
        return next_stab, my_stab, my_decay, my_weight

    gain_copy.wait()
    cell_copies = fetch_cell(0)
    tok_copy.wait()
    current = tok_buf[...].astype(jnp.float32)
    mean = jnp.sum(current * current, axis=-1, keepdims=True) * (1.0 / width)
    normed = (current * lax.rsqrt(mean + epsilon) * gain_buf[0:1, :]).astype(jnp.bfloat16)
    weight_copies[0].wait()
    weight_copies[1].wait()
    both = lax.dot_general(
        normed, weights[: 2 * ncols], NT, preferred_element_type=jnp.float32
    )
    pair_buf[core, 0] = both[:, :ncols].astype(jnp.bfloat16)
    key = (both[:, ncols:] * dh ** (-0.5)).astype(jnp.bfloat16)
    pair_buf[core, 1] = key
    weight_copies[2].wait()
    weight_copies[3].wait()
    for copy in small:
        copy.wait()
    norm_copy.wait()
    pl.semaphore_wait(barrier, n - 1)
    pair_copies = [
        push(pair_buf.at[core], pair_buf.at[core], partner, pair_send.at[0], pair_recv.at[0]),
        push(norm_buf.at[core], norm_buf.at[core], partner, pair_send.at[1], pair_recv.at[1]),
    ]
    both = lax.dot_general(
        normed, weights[2 * ncols :], NT, preferred_element_type=jnp.float32
    )
    value = both[:, :ncols].astype(jnp.bfloat16).astype(jnp.float32)
    gate = jax.nn.sigmoid(both[:, ncols:].astype(jnp.bfloat16).astype(jnp.float32))
    gates = lax.dot_general(normed, gate_buf[0], NT, preferred_element_type=jnp.float32)
    next_stab, my_stab, my_decay, my_weight = scale(gates, 0, stab_buf[0].T)
    new_stab[0] = next_stab.T
    new_norm[0] = my_decay * norm_buf[core, 0] + my_weight * key.astype(jnp.float32)
    weighted = my_weight * value
    arrived(pair_buf.at[1 - core], pair_recv.at[0])
    arrived(norm_buf.at[1 - core], pair_recv.at[1])
    q_head = jnp.concatenate([pair_buf[j, 0] for j in range(2)], axis=1).astype(jnp.float32)
    k_head = jnp.concatenate([pair_buf[j, 1] for j in range(2)], axis=1).astype(jnp.float32)
    n_head = jnp.concatenate([norm_buf[j, 0] for j in range(2)], axis=1)
    inner = jnp.sum(q_head * k_head, axis=-1, keepdims=True)
    den = bound(q_head, k_head, n_head, my_stab, my_decay, my_weight)

    branch_copies = []
    for h in range(2):
        for c in range(h * CELL_CHUNKS // 2, (h + 1) * CELL_CHUNKS // 2):
            cell_copies[c].wait()
        if h == 1:
            proj_copies = [fetch(w_proj.at[0], own_rows(proj_buf, 0), small_sem.at[6])]
            wide_copies = [
                fetch(names[i].at[1], own_rows(wide, i), wide_sem.at[i]) for i in range(4)
            ]
            proj_copies.append(fetch(w_proj.at[1], own_rows(proj_out, 0), small_sem.at[7]))
        for c in range(h * CELL_CHUNKS // 2, (h + 1) * CELL_CHUNKS // 2):
            queries = jnp.concatenate(
                [pair_buf[j, 0, pl.ds(c * rows, rows), :] for j in range(2)], axis=1
            )
            read_rows(lambda b: cell_buf[0, b], queries, numer_buf, c * rows, rows)
        part = slice(h * half, (h + 1) * half)
        numer = my_decay[part] * numer_buf[part, :] + weighted[part] * inner[part]
        send_buf[part, :] = (gate[part] * (numer / den[part])).astype(jnp.bfloat16)
        branch_copies += send_half(
            h, chip, core, chips, half, send_buf, branch_buf, branch_send, branch_recv
        )
    branch_copies.append(
        send_across(chip, core, half, send_buf, branch_buf, branch_send, branch_recv)
    )
    proj_copies[0].wait()
    pair_copies.append(
        push(own_rows(proj_buf, 0), own_rows(proj_buf, 0), partner, pair_send.at[2], pair_recv.at[2])
    )
    wide_pushes = []
    for i in range(4):
        wide_copies[i].wait()
        wide_pushes.append(
            push(
                own_rows(wide, i),
                own_rows(wide, i),
                partner,
                pair_send.at[3 + i],
                pair_recv.at[3 + i],
            )
        )
    cell_copies = fetch_cell(1)
    proj_copies[1].wait()
    pair_copies.append(
        push(own_rows(proj_out, 0), own_rows(proj_out, 0), partner, pair_send.at[9], pair_recv.at[9])
    )
    arrived(
        proj_buf.at[pl.ds(pl.multiple_of((1 - core) * ncols, ncols), ncols)], pair_recv.at[2]
    )
    summed = gather_project(chip, core, chips, half, branch_buf, branch_recv, proj_buf)
    my_rows = pl.ds(pl.multiple_of(core * half, half), half)
    my_cols = pl.ds(pl.multiple_of(chip * 2 * ncols, 2 * ncols), 2 * ncols)
    result = (tok_buf[my_rows, my_cols].astype(jnp.float32) + summed).astype(jnp.bfloat16)
    own_out[...] = result
    result_out[...] = result
    result_copies = [
        push(
            result_out,
            result_buf.at[chip],
            flip(chip, m) * 2 + 1 - core,
            result_send.at[m],
            result_recv.at[m],
        )
        for m in sending_order(chips)
    ]

    update_rows(cell_buf.at[0], my_decay, weighted, k_head)
    one_out[...] = jnp.ones_like(one_out)
    for i in range(4):
        arrived(
            wide.at[pl.ds(pl.multiple_of(i * 2 * ncols + (1 - core) * ncols, ncols), ncols)],
            pair_recv.at[3 + i],
        )
    total = jnp.zeros((half, 8 * ncols), jnp.float32)
    gates = jnp.zeros((half, 2 * heads), jnp.float32)
    square = jnp.zeros((half, 1), jnp.float32)
    for other, m, _ in landing_order(chip, chips):
        arrived(result_buf.at[other], result_recv.at[m])
        cols = pl.ds(pl.multiple_of(other * 2 * ncols, 2 * ncols), 2 * ncols)
        block = result_buf[other].astype(jnp.float32)
        square = square + jnp.sum(block * block, axis=-1, keepdims=True)
        block = (block * gain_buf[1:2, cols]).astype(jnp.bfloat16)
        total = total + lax.dot_general(
            block, wide[:, cols], NT, preferred_element_type=jnp.float32
        )
        gates = gates + lax.dot_general(
            block, gate_buf[1, :, cols], NT, preferred_element_type=jnp.float32
        )
    root = lax.rsqrt(square * (1.0 / width) + epsilon)
    old_stab = jnp.where(core == 0, stab_buf[1].T[half:], stab_buf[1].T[:half])
    scalars = scale(gates * root, 1, old_stab)
    gates_buf[1 - core] = jnp.concatenate(
        scalars + (jnp.zeros((half, ncols - heads - 3), jnp.float32),), axis=1
    )
    total = total * root
    query = total[:, : 2 * ncols].astype(jnp.bfloat16)
    key = (total[:, 2 * ncols : 4 * ncols] * dh ** (-0.5)).astype(jnp.bfloat16)
    whole_buf[...] = total[:, 4 * ncols :].astype(jnp.bfloat16)
    for target, side in ((swap_out, 1 - core), (swap_buf.at[1 - core], core)):
        target[:, : 2 * ncols] = query
        target[:, 2 * ncols : 4 * ncols] = key
        for i in range(2):
            target[:, (4 + i) * ncols : (5 + i) * ncols] = whole_buf[
                :, pl.ds(pl.multiple_of(i * 2 * ncols + side * ncols, ncols), ncols)
            ]
    pair_copies += [
        push(swap_out, swap_buf.at[1 - core], partner, pair_send.at[7], pair_recv.at[7]),
        push(
            gates_buf.at[1 - core],
            gates_buf.at[1 - core],
            partner,
            pair_send.at[8],
            pair_recv.at[8],
        ),
    ]
    for j in range(2):
        norm_out[j] = norm_buf[j, 1]
    for copy in cell_copies:
        copy.wait()

    def update_half(side):
        scalars = gates_buf[side]
        my_decay = scalars[:, heads + 1 : heads + 2]
        my_weight = scalars[:, heads + 2 : heads + 3]
        keys = swap_buf[side, :, 2 * ncols : 4 * ncols].astype(jnp.float32)
        value = swap_buf[side, :, 4 * ncols : 5 * ncols].astype(jnp.float32)
        cells = cell_buf.at[1, pl.ds(side * half, half)]
        update_rows(cells, my_decay, my_weight * value, keys)

    update_half(1 - core)
    for copy in branch_copies + wide_pushes + result_copies:
        copy.wait_send()
    arrived(
        proj_out.at[pl.ds(pl.multiple_of((1 - core) * ncols, ncols), ncols)], pair_recv.at[9]
    )
    arrived(swap_buf.at[core], pair_recv.at[7])
    arrived(gates_buf.at[core], pair_recv.at[8])
    update_half(core)

    def both_halves(part):
        return jnp.concatenate([swap_buf[j, :, part] for j in range(2)], axis=0)

    scalars = jnp.concatenate([gates_buf[j] for j in range(2)], axis=0)
    scale_out[...] = scalars
    new_stab[1] = scalars[:, :heads].T
    my_decay = scalars[:, heads + 1 : heads + 2]
    my_weight = scalars[:, heads + 2 : heads + 3]
    q_out[...] = both_halves(slice(0, 2 * ncols))
    key_out[...] = both_halves(slice(2 * ncols, 4 * ncols))
    gate_out[...] = both_halves(slice(5 * ncols, 6 * ncols))
    key = both_halves(pl.ds(pl.multiple_of((2 + core) * ncols, ncols), ncols))
    new_norm[1] = my_decay * norm_buf[core, 1] + my_weight * key.astype(jnp.float32)
    for copy in pair_copies:
        copy.wait_send()


def last_kernel(
    n,
    heads,
    cell_buf,
    queries,
    keys,
    norms,
    scalars,
    outgate,
    own,
    proj_buf,
    _,
    mixed,
    send_buf,
    branch_buf,
    swap_buf,
    swap_out,
    numer_buf,
    pair_send,
    pair_recv,
    branch_send,
    branch_recv,
):
    layers, batch, ncols, dh = cell_buf.shape
    last = layers - 1
    rows = batch // CELL_CHUNKS
    half = batch // 2
    chips = n // 2
    me = lax.axis_index("tp")
    core = lax.rem(me, 2)
    chip = lax.div(me, 2)
    partner = chip * 2 + 1 - core
    barrier = greet_all(n, me)
    for c in range(CELL_CHUNKS):
        read_rows(
            lambda b: cell_buf[last, b],
            queries[pl.ds(c * rows, rows), :],
            numer_buf,
            c * rows,
            rows,
        )
    q_head = queries[...].astype(jnp.float32)
    n_head = jnp.concatenate([norms[j] for j in range(2)], axis=1)
    my_stab, my_decay, my_weight = (scalars[:, heads + i : heads + i + 1] for i in range(3))
    den = bound(q_head, keys[...].astype(jnp.float32), n_head, my_stab, my_decay, my_weight)
    gate = jax.nn.sigmoid(outgate[...].astype(jnp.float32))
    send_buf[...] = (gate * (numer_buf[...] / den)).astype(jnp.bfloat16)
    pl.semaphore_wait(barrier, n - 1)
    copies = [
        push(
            send_buf.at[pl.ds(h * half, half)],
            branch_buf.at[me],
            target * 2 + h,
            branch_send.at[h, m],
            branch_recv.at[m, core],
        )
        for target, m in first_to_zero(chip, chips)
        for h in range(2)
    ]
    copies.append(send_across(chip, core, half, send_buf, branch_buf, branch_send, branch_recv))
    summed = gather_project(chip, core, chips, half, branch_buf, branch_recv, proj_buf)
    result = (own[...].astype(jnp.float32) + summed).astype(jnp.bfloat16)
    swap_buf[...] = result
    swap_out[core] = swap_buf[:, pl.ds(pl.multiple_of((1 - core) * ncols, ncols), ncols)]
    swap_copy = push(swap_out.at[core], swap_out.at[2 + core], partner, pair_send, pair_recv)
    mixed[pl.ds(pl.multiple_of(core * half, half), half), :] = swap_buf[
        :, pl.ds(pl.multiple_of(core * ncols, ncols), ncols)
    ]
    for copy in copies:
        copy.wait_send()
    arrived(swap_out.at[3 - core], pair_recv)
    mixed[pl.ds(pl.multiple_of((1 - core) * half, half), half), :] = swap_out[3 - core]
    swap_copy.wait_send()


def fused_body(n, *args):
    (tokens, norm_gain, w_query, _, _, _, w_gates, bias_forget, _, cell, norm_vec, stab) = args
    layers, batch, ncols, dh = cell.shape
    width = tokens.shape[1]
    half = batch // 2
    chips = n // 2
    w_gates = jnp.swapaxes(w_gates, 1, 2)
    stab = jnp.swapaxes(stab, 1, 2)
    args = args[:6] + (w_gates,) + args[7:11] + (stab,)
    args = [pltpu.with_memory_space_constraint(arg, pltpu.HBM) for arg in args]
    bf16, f32 = jnp.bfloat16, jnp.float32
    vmem = pl.BlockSpec(memory_space=pltpu.VMEM)
    hbm = pl.BlockSpec(memory_space=pltpu.HBM)
    dma = pltpu.SemaphoreType.DMA
    held, new_norm, new_stab, one, *rest = pl.pallas_call(
        functools.partial(cells_kernel, n),
        out_shape=(
            pltpu.VMEM(cell.shape, f32),
            jax.ShapeDtypeStruct(norm_vec.shape, f32),
            jax.ShapeDtypeStruct(stab.shape, f32),
            jax.ShapeDtypeStruct((1, dh), f32),
            jax.ShapeDtypeStruct((batch, dh), bf16),
            jax.ShapeDtypeStruct((batch, dh), bf16),
            jax.ShapeDtypeStruct((2, batch, ncols), f32),
            jax.ShapeDtypeStruct((batch, ncols), f32),
            jax.ShapeDtypeStruct((batch, ncols), bf16),
            jax.ShapeDtypeStruct((half, dh), bf16),
            jax.ShapeDtypeStruct((2 * ncols, width), bf16),
        ),
        in_specs=[hbm] * len(args),
        out_specs=(vmem,) * 11,
        scratch_shapes=[
            pltpu.VMEM(tokens.shape, bf16),
            pltpu.VMEM(norm_gain.shape, f32),
            pltpu.VMEM((4 * ncols, width), bf16),
            pltpu.VMEM((8 * ncols, width), bf16),
            pltpu.VMEM((2 * ncols, width), bf16),
            pltpu.VMEM(w_gates.shape, bf16),
            pltpu.VMEM(bias_forget.shape, f32),
            pltpu.VMEM(stab.shape, f32),
            pltpu.VMEM((2,) + norm_vec.shape, f32),
            pltpu.VMEM((2, 2, batch, ncols), bf16),
            pltpu.VMEM((batch, ncols), bf16),
            pltpu.VMEM((n, half, ncols), bf16),
            pltpu.VMEM((chips, half, 2 * ncols), bf16),
            pltpu.VMEM((half, 2 * ncols), bf16),
            pltpu.VMEM((half, 4 * ncols), bf16),
            pltpu.VMEM((2, half, 6 * ncols), bf16),
            pltpu.VMEM((half, 6 * ncols), bf16),
            pltpu.VMEM((2, half, ncols), f32),
            pltpu.VMEM((batch, ncols), f32),
            dma((8,)),
            dma((4,)),
            dma((4,)),
            dma((layers, CELL_CHUNKS)),
            dma((10,)),
            dma((10,)),
            dma((2, chips)),
            dma((chips, 2)),
            dma((chips,)),
            dma((chips,)),
        ],
        compiler_params=pltpu.CompilerParams(
            collective_id=0, has_side_effects=True, vmem_limit_bytes=MAIN_VMEM
        ),
        name="cells",
    )(*args)
    new_cell = held * one[0]
    keys, queries, norms, scalars, outgate, own, proj = rest
    mixed = pl.pallas_call(
        functools.partial(last_kernel, n, stab.shape[1]),
        out_shape=jax.ShapeDtypeStruct((batch, ncols), bf16),
        in_specs=[vmem] * 9,
        out_specs=vmem,
        scratch_shapes=[
            pltpu.VMEM((batch, ncols), bf16),
            pltpu.VMEM((n, half, ncols), bf16),
            pltpu.VMEM((half, 2 * ncols), bf16),
            pltpu.VMEM((4, half, ncols), bf16),
            pltpu.VMEM((batch, ncols), f32),
            dma,
            dma,
            dma((2, chips)),
            dma((chips, 2)),
        ],
        compiler_params=pltpu.CompilerParams(
            collective_id=1, has_side_effects=True, vmem_limit_bytes=LAST_VMEM
        ),
        cost_estimate=pl.CostEstimate(
            flops=5 * 10**10, bytes_accessed=10**6, transcendentals=0
        ),
        name="last",
    )(
        held,
        queries,
        keys,
        norms,
        scalars,
        outgate,
        own,
        proj,
        new_cell[0, 0, :8, :128],
    )
    mixed, new_norm, new_stab = write_small(mixed, new_norm, new_stab)
    return mixed, new_cell, new_norm, jnp.swapaxes(new_stab, 1, 2)


def write_kernel(*refs):
    half = len(refs) // 2
    sems = refs[-1]
    copies = [
        pltpu.make_async_copy(refs[i], refs[half + i], sems.at[i]) for i in range(half)
    ]
    for copy in copies:
        copy.start()
    for copy in copies:
        copy.wait()


def write_small(*arrays):
    return pl.pallas_call(
        write_kernel,
        out_shape=[jax.ShapeDtypeStruct(x.shape, x.dtype) for x in arrays],
        in_specs=[pl.BlockSpec(memory_space=pltpu.VMEM)] * len(arrays),
        out_specs=[pl.BlockSpec(memory_space=pltpu.HBM)] * len(arrays),
        scratch_shapes=[pltpu.SemaphoreType.DMA((len(arrays),))],
        compiler_params=pltpu.CompilerParams(vmem_limit_bytes=2**20),
        name="write",
    )(*arrays)


def whole_body(*args):
    n = lax.axis_size("tp")
    layers, batch, ncols, dh = args[9].shape
    heads = args[11].shape[2]
    if (
        layers == 2
        and n == 2 * heads
        and n & (n - 1) == 0
        and ncols % 128 == 0
        and dh == 2 * ncols
        and batch % (16 * CELL_CHUNKS) == 0
    ):
        return fused_body(n, *args)
    return body(*args)


def solution(mesh):
    return jax.shard_map(
        whole_body,
        mesh=mesh,
        in_specs=(
            P("grp", None),
            P(),
            P(None, "tp", None),
            P(None, "tp", None),
            P(None, "tp", None),
            P(None, "tp", None),
            P(),
            P(),
            P(None, "tp", None),
            P(None, "grp", "tp", None),
            P(None, "grp", "tp"),
            P(None, "grp", None),
        ),
        out_specs=(
            P("grp", "tp"),
            P(None, "grp", "tp", None),
            P(None, "grp", "tp"),
            P(None, "grp", None),
        ),
        check_vma=False,
    )
```
